512 devices in a mesh: grp: 2 (over y), dp: 8 (over x), kv: 16 (over z), tp: 2 (over core).
Axes of the slice: x: 8, y: 2, z: 16, core: 2. Of those that a mesh axis runs over, the one named last changes fastest.
The devices are a block of a 8x8x16 slice.
Arguments:
- tokens: bfloat16 [16, 6144, 2048], P(('grp', 'dp'), 'kv'), parts along dimension 0, may hold values from -14 to 14
- query_weight: bfloat16 [2048, 1024], P('kv', 'tp'), may hold values from -0.1875 to 0.1875
- key_weight: bfloat16 [2048, 512], P('kv', 'tp'), may hold values from -0.1875 to 0.1875
- value_weight: bfloat16 [2048, 512], P('kv', 'tp'), may hold values from -0.125 to 0.125
- output_weight: bfloat16 [1024, 2048], P('tp', 'kv'), may hold values from -3.59375 to 3.59375
- block_choice: int32 [16, 96, 16], P(('grp', 'dp'), 'kv'), parts along dimension 0, may hold values from -1 to 95, as said below
Outputs:
- attention: bfloat16 [16, 6144, 2048], P(('grp', 'dp'), 'kv', 'tp'), parts along dimension 0
The draws below stay inside these ranges and needn't reach their ends.
There are 2 independent parts, one for each index of `grp`. The reference program is written for one: setup_inputs(seed, part) draws one part's arguments, and reference() takes and returns one part's arrays. A program takes and returns all parts, laid end to end along the dimension named above; an argument that names none is the same for every part. Nothing has to cross between parts.
Inputs may be any that keep to these rules, and one draw needn't show every extreme that they name: `block_choice`: row i of a sequence names distinct key blocks below i, the named ones first and -1 in the slots after them. Split the rows into aligned groups of 6 (the query blocks that share one index of kv, whose key blocks are the same 6 blocks): the rows of one group name at most 4 distinct blocks among those of any other group, and every row of a group names all of exactly 4 blocks of the group just before it.
All inputs are finite; a program needn't handle non-finite values.
Results may differ from the reference program's by a relative error of at most 0.012.
Values may be sent and summed in bfloat16 or wider, within the bound.
No kernel may reach another device: no remote copies, remote signals or barrier semaphores. Data moves between devices by JAX's collectives and lax.ppermute only.
A program may use at most 64 MiB of HBM per device.

```python
import jax
import jax.numpy as jnp
from jax import lax

D = 2048
HEADS = 8
KV_HEADS = 4
HEAD = 128
BLOCK = 64
NSEL = 16
CAP = 4
SEQS = 8
LENGTH = 6144
NBLK = 96
QBLK = 6
PARTIALS = 2


def weights_pair(key):
    query_key, noise_key = jax.random.split(jax.random.fold_in(key, 71))
    query_part = jnp.clip(jax.random.normal(query_key, (D, HEADS * HEAD), jnp.float32) * D ** (-0.5), -0.1875, 0.1875)
    noise_part = jnp.clip(jax.random.normal(noise_key, (D, KV_HEADS * HEAD), jnp.float32) * D ** (-0.5), -0.1875, 0.1875)
    return (query_part, noise_part)


def draw_query_weight(key, part):
    query_part, noise_part = weights_pair(key)
    return query_part.astype(jnp.bfloat16)


def draw_key_weight(key, part):
    query_part, noise_part = weights_pair(key)
    return noise_part.astype(jnp.bfloat16)


def draw_tokens(key, part):
    base_key, scale_key = jax.random.split(jax.random.fold_in(key, 13))
    base = jax.random.normal(base_key, (SEQS, LENGTH, D), jnp.float32)
    return jnp.clip(base, -14.0, 14.0).astype(jnp.bfloat16)


def draw_block_choice(key, part):
    owners = NBLK // QBLK
    popular_key, noise_key, priority_key = jax.random.split(jax.random.fold_in(key, 29), 3)
    local_iota = jnp.arange(QBLK, dtype=jnp.int32)
    owner_iota = jnp.arange(owners, dtype=jnp.int32)
    popular = jax.random.randint(popular_key, (SEQS, 1, owners, QBLK), 0, 3) * 4096
    noise_draw = jax.random.randint(noise_key, (SEQS, owners, owners, QBLK), 0, 4096)
    ranking = (noise_draw + popular) * QBLK + local_iota
    chosen_local = lax.top_k(ranking, CAP)[1].astype(jnp.int32)
    remote_ids = (owner_iota[None, None, :, None] * QBLK + chosen_local).reshape(SEQS, owners, owners * CAP)
    remote_owner = jnp.repeat(owner_iota, CAP)
    remote_slot = jnp.tile(jnp.arange(CAP, dtype=jnp.int32), owners)
    requester = owner_iota[:, None]
    remote_valid = remote_owner[None, :] < requester
    forced = (remote_owner[None, :] == requester - 1) | (remote_owner[None, :] == requester - owners // 2) & (remote_slot[None, :] == 0)
    local_ids = requester * QBLK + local_iota[None, :]
    candidates = owners * CAP + QBLK
    id_grid = jnp.concatenate([jnp.broadcast_to(remote_ids[:, :, None, :], (SEQS, owners, QBLK, owners * CAP)), jnp.broadcast_to(local_ids[None, :, None, :], (SEQS, owners, QBLK, QBLK))], axis=3)
    local_valid = jnp.broadcast_to(local_iota[None, None, :] < local_iota[None, :, None], (owners, QBLK, QBLK))
    valid_grid = jnp.concatenate([jnp.broadcast_to(remote_valid[:, None, :], (owners, QBLK, owners * CAP)), local_valid], axis=2)
    forced_grid = jnp.concatenate([jnp.broadcast_to(forced[:, None, :], (owners, QBLK, owners * CAP)), jnp.zeros((owners, QBLK, QBLK), bool)], axis=2)
    priority = jax.random.randint(priority_key, (SEQS, owners, QBLK, candidates), 0, 65536)
    column_iota = jnp.arange(candidates, dtype=jnp.int32)
    ranked = jnp.where(valid_grid, (forced_grid.astype(jnp.int32) * 131072 + priority + 1) * candidates + column_iota, -1 - column_iota)
    best_score, best_index = lax.top_k(ranked, NSEL)
    picked = jnp.take_along_axis(id_grid, best_index.astype(jnp.int32), axis=3)
    result = jnp.where(best_score >= 0, picked, -1)
    return result.reshape(SEQS, NBLK, NSEL).astype(jnp.int32)


def steps_of(own_key, dims, pieces, least, top_value):
    level, own = 1.0, jax.random.fold_in(own_key, 6)
    for axis_at, blocks in pieces:
        heights = jnp.exp(jax.random.uniform(jax.random.fold_in(own, axis_at), (blocks,), jnp.float32, least / len(pieces), top_value / len(pieces)))
        level = level * jnp.repeat(heights, dims[axis_at] // blocks).reshape([-1 if axis == axis_at else 1 for axis in range(len(dims))])
    return level


def scatter_about(own_key, extent, spread, reach, cuts=(), kind=jnp.bfloat16):
    values = jax.random.normal(own_key, extent, jnp.float32) * spread
    if len(cuts) > 0:
        values = steps_of(own_key, extent, cuts, -0.22, 0.18) * values
    return jnp.clip(values, min=-reach, max=reach).astype(kind)


def setup_inputs(seed: int = 0, part: int = 0) -> dict:
    arg_keys = jax.random.split(jax.random.key(seed), 7)
    own_keys = jax.random.split(jax.random.fold_in(arg_keys[6], part), 7)
    tokens = draw_tokens(jax.random.fold_in(jax.random.fold_in(arg_keys[6], part), 71), part)
    query_weight = draw_query_weight(jax.random.fold_in(arg_keys[6], 71), part)
    key_weight = draw_key_weight(jax.random.fold_in(arg_keys[6], 71), part)
    value_weight = scatter_about(arg_keys[3], (D, KV_HEADS * HEAD), D ** -0.5, 0.125, ((0, 16), (1, 2)))
    output_weight = scatter_about(arg_keys[4], (HEADS * HEAD, D), 0.6, 3.59375, ((0, 2), (1, 16)))
    block_choice = draw_block_choice(jax.random.fold_in(jax.random.fold_in(arg_keys[6], part), 71), part)
    return dict(tokens=tokens, query_weight=query_weight, key_weight=key_weight, value_weight=value_weight, output_weight=output_weight, block_choice=block_choice)


THETA = 10000.0
NEGATIVE = -1e30


def rotate(field_rows, positions):
    half_width = HEAD // 2
    inverse = THETA ** (-jnp.arange(half_width, dtype=jnp.float32) / half_width)
    angles = positions.astype(jnp.float32)[:, None] * inverse[None, :]
    cosine = jnp.cos(angles)[:, None, :]
    sine_rows = jnp.sin(angles)[:, None, :]
    first_half = field_rows[..., :half_width]
    second = field_rows[..., half_width:]
    return jnp.concatenate([first_half * cosine - second * sine_rows, second * cosine + first_half * sine_rows], axis=-1)


def one_sequence(features, choice_rows, query_weight, key_weight, value_weight, output_weight):
    positions = jnp.arange(LENGTH, dtype=jnp.int32)
    group_size = HEADS // KV_HEADS
    query_full = jnp.dot(features, query_weight, preferred_element_type=jnp.float32).reshape(LENGTH, HEADS, HEAD)
    queries = lax.optimization_barrier(rotate(query_full, positions).astype(jnp.bfloat16))
    key_full = jnp.dot(features, key_weight, preferred_element_type=jnp.float32).reshape(LENGTH, KV_HEADS, HEAD)
    key_rows = lax.optimization_barrier(rotate(key_full, positions).astype(jnp.bfloat16))
    value_rows = lax.optimization_barrier(jnp.dot(features, value_weight, preferred_element_type=jnp.float32).astype(jnp.bfloat16))
    query_blocks = queries.reshape(NBLK, BLOCK, KV_HEADS, group_size, HEAD)
    key_blocks = key_rows.reshape(NBLK, BLOCK, KV_HEADS, HEAD)
    value_blocks = value_rows.reshape(NBLK, BLOCK, KV_HEADS, HEAD)
    offsets = jnp.arange(BLOCK, dtype=jnp.int32)
    causal = offsets[None, :] <= offsets[:, None]

    def attend(block_index):
        chosen_row = choice_rows[block_index]
        listed = chosen_row >= 0
        picked = jnp.maximum(chosen_row, 0)
        near_keys = jnp.concatenate([key_blocks[picked].reshape(NSEL * BLOCK, KV_HEADS, HEAD), key_blocks[block_index]], axis=0)
        near_values = jnp.concatenate([value_blocks[picked].reshape(NSEL * BLOCK, KV_HEADS, HEAD), value_blocks[block_index]], axis=0)
        listed_keys = jnp.broadcast_to(jnp.repeat(listed, BLOCK)[None, :], (BLOCK, NSEL * BLOCK))
        visible = jnp.concatenate([listed_keys, causal], axis=1)
        scores = jnp.einsum("qgrd,kgd->grqk", query_blocks[block_index].astype(jnp.float32), near_keys.astype(jnp.float32)) * HEAD ** -0.5
        scores = jnp.where(visible[None, None], scores, NEGATIVE)
        row_top = jnp.max(scores, axis=-1, keepdims=True)
        weights = jnp.exp(scores - row_top)
        row_total = jnp.sum(weights, axis=-1)
        rounded = lax.optimization_barrier(weights.astype(jnp.bfloat16))
        weighted = jnp.einsum("grqk,kgd->qgrd", rounded.astype(jnp.float32), near_values.astype(jnp.float32))
        weighted = weighted / jnp.transpose(row_total, (2, 0, 1))[..., None]
        return weighted.astype(jnp.bfloat16)

    mixed = lax.map(attend, jnp.arange(NBLK, dtype=jnp.int32)).reshape(LENGTH, HEADS * HEAD)
    part_width = HEADS * HEAD // PARTIALS
    summed = jnp.zeros((LENGTH, D), jnp.float32)
    for part_index in range(PARTIALS):
        columns = mixed[:, part_index * part_width:(part_index + 1) * part_width]
        piece_out = jnp.dot(columns, output_weight[part_index * part_width:(part_index + 1) * part_width], preferred_element_type=jnp.float32)
        summed = summed + lax.optimization_barrier(piece_out.astype(jnp.bfloat16)).astype(jnp.float32)
    return summed.astype(jnp.bfloat16)


def reference(tokens, query_weight, key_weight, value_weight, output_weight, block_choice):
    def per_sequence(inputs):
        return one_sequence(inputs[0], inputs[1], query_weight, key_weight, value_weight, output_weight)

    return lax.map(per_sequence, (tokens, block_choice))
```

```python
import functools

import jax
import jax.numpy as jnp
from jax import lax
from jax.experimental import pallas as pl
from jax.experimental.pallas import tpu as pltpu
from jax.sharding import PartitionSpec as P

HEAD = 128
BLOCK = 64
THETA = 10000.0
NEGATIVE = -1e30
LOG2E = 1.4426950408889634

bf16, f32 = jnp.bfloat16, jnp.float32
VMEM = pl.BlockSpec(memory_space=pltpu.VMEM)
SMEM = pl.BlockSpec(memory_space=pltpu.SMEM)


def call(kernel, outs, args, scratch=(), flops=0, moved=0):
    return pl.pallas_call(
        kernel,
        out_shape=[jax.ShapeDtypeStruct(s, d) for s, d in outs],
        in_specs=[SMEM] + [VMEM] * (len(args) - 1),
        out_specs=[VMEM] * len(outs),
        scratch_shapes=list(scratch),
        compiler_params=pltpu.CompilerParams(vmem_limit_bytes=24 * 2**20),
        cost_estimate=pl.CostEstimate(flops=flops, bytes_accessed=moved, transcendentals=0),
    )(*args)


def shift(axis, by):
    n = lax.axis_size(axis)
    return [(i, (i + by) % n) for i in range(n)]


def rings(starts, axis):
    n = lax.axis_size(axis)
    got = [[(0, x)] for x in starts]
    right, left = list(starts), list(starts)
    for k in range(1, n // 2 + 1):
        for s in range(len(starts)):
            if k < n // 2 or s % 2 == 0:
                right[s] = lax.ppermute(right[s], axis, shift(axis, 1))
                got[s].append((-k, right[s]))
            if k < n // 2 or s % 2 == 1:
                left[s] = lax.ppermute(left[s], axis, shift(axis, -1))
                got[s].append((k, left[s]))
    return got


def turned(u, cos, sin):
    return u * cos + pltpu.roll(u, HEAD // 2, 1) * sin


def kv_kernel(offsets, n, me, x, cos, sin, *refs):
    chunks, (kv_out, slice_out, w) = refs[: len(offsets)], refs[len(offsets) :]
    for off, chunk in zip(offsets, chunks):
        src = lax.rem(me[0] + (off + n), n)
        rows = pl.ds(pl.multiple_of(src * HEAD, HEAD), HEAD)
        w[rows, 0:HEAD] = chunk[0:HEAD, :]
        w[rows, HEAD : 2 * HEAD] = chunk[HEAD : 2 * HEAD, :]
        slice_out[src] = chunk[2 * HEAD :, :]
    y = jnp.dot(x[...], w[...], preferred_element_type=f32)
    kv_out[0] = turned(y[:, :HEAD], cos[...], sin[...]).astype(bf16)
    kv_out[1] = y[:, HEAD:].astype(bf16)


def q_kernel(offsets, n, me, x, cos, sin, *refs):
    pieces, (q_out, w) = refs[: len(offsets)], refs[len(offsets) :]
    heads = w.shape[2] // HEAD
    parts = n // heads
    part_rows = HEAD // parts
    for off, piece in zip(offsets, pieces):
        src = lax.rem(me[0] + (off + n), n)
        t, low = src // parts, lax.rem(src, parts)
        w[:, pl.ds(pl.multiple_of(low * part_rows, part_rows), part_rows), pl.ds(pl.multiple_of(t * HEAD, HEAD), HEAD)] = piece[...]
    groups, blocks = q_out.shape[0], q_out.shape[1]
    rep = heads // groups
    whole = w[...].reshape(w.shape[0] * HEAD, heads * HEAD)
    y = jnp.dot(x[...], whole, preferred_element_type=f32)
    for t in range(heads):
        u = turned(y[:, t * HEAD : (t + 1) * HEAD], cos[...], sin[...]).astype(bf16)
        r = t % rep
        q_out[t // rep, :, r * BLOCK : (r + 1) * BLOCK, :] = u.reshape(blocks, BLOCK, HEAD)


def attend_kernel(group, offsets, n, first, last, me, bias, q, *refs):
    count = len(offsets)
    if not first:
        (m_in, l_in, acc_in), refs = refs[:3], refs[3:]
    kvs, refs = refs[:count], refs[count:]
    blocks, rows = q.shape[1], q.shape[2]
    keys = kvs[0].shape[1]
    scale = HEAD ** (-0.5) * LOG2E
    if last:
        out, s_ref = refs
    else:
        m_out, l_out, acc_out, s_ref = refs
    lane_tiles = keys // HEAD

    def body(i, _):
        qi = q[group, i]
        running = None
        for j, (off, kv) in enumerate(zip(offsets, kvs)):
            src = lax.rem(me[0] + (off + n), n)
            s = lax.dot_general(qi, kv[0], (((1,), (1,)), ((), ())), preferred_element_type=f32)
            s = s * scale + bias[pl.ds(i * n + src, 1), :]
            if off == 0:
                col = lax.broadcasted_iota(jnp.int32, s.shape, 1)
                row = lax.broadcasted_iota(jnp.int32, s.shape, 0)
                s = jnp.where(col <= i * BLOCK + lax.rem(row, BLOCK), s, NEGATIVE)
            s_ref[:, j * keys : (j + 1) * keys] = s
            for c in range(lane_tiles):
                tile = s[:, c * HEAD : (c + 1) * HEAD]
                running = tile if running is None else jnp.maximum(running, tile)
        top = jnp.broadcast_to(jnp.max(running, axis=1, keepdims=True), (rows, HEAD))
        if first:
            m, total, acc = top, jnp.zeros((rows, HEAD), f32), jnp.zeros((rows, HEAD), f32)
        else:
            m = jnp.maximum(m_in[i], top)
            fade = jnp.exp2(m_in[i] - m)
            total, acc = l_in[i] * fade, acc_in[i] * fade
        for j, kv in enumerate(kvs):
            p = jnp.concatenate(
                [jnp.exp2(s_ref[:, j * keys + c * HEAD : j * keys + (c + 1) * HEAD] - m) for c in range(lane_tiles)], axis=1
            )
            for c in range(lane_tiles):
                total = total + p[:, c * HEAD : (c + 1) * HEAD]
            acc = acc + jnp.dot(p.astype(bf16), kv[1], preferred_element_type=f32)
        if last:
            mixed = (acc / jnp.sum(total, axis=1, keepdims=True)).astype(bf16)
            for r in range(rows // BLOCK):
                out[pl.ds(pl.multiple_of(i * BLOCK, BLOCK), BLOCK), r * HEAD : (r + 1) * HEAD] = mixed[r * BLOCK : (r + 1) * BLOCK]
        else:
            m_out[i], l_out[i], acc_out[i] = m, total, acc
        return 0

    lax.fori_loop(0, blocks, body, 0)


def order_kernel(offsets, n, me, *refs):
    pieces, (theirs, ours) = refs[: len(offsets)], refs[len(offsets) :]
    for off, piece in zip(offsets, pieces):
        src = lax.rem(me[0] + (off + n), n)
        depth = piece.shape[1]
        half = piece.shape[0] // 2
        rows = pl.ds(pl.multiple_of(src * depth, depth), depth)
        for c in range(half):
            theirs[rows, c * HEAD : (c + 1) * HEAD] = piece[(1 - me[1]) * half + c]
            ours[rows, c * HEAD : (c + 1) * HEAD] = piece[me[1] * half + c]


def term_kernel(me, *refs):
    parts, (w, out) = refs[:-2], refs[-2:]
    mixed = jnp.concatenate([p[...] for p in parts], axis=1)
    out[...] = jnp.dot(mixed, w[...], preferred_element_type=f32).astype(bf16)


def on_device(tokens, query_weight, key_weight, value_weight, output_weight, block_choice):
    x = tokens[0]
    row_count, width = x.shape
    n, nx = lax.axis_size("kv"), lax.axis_size("dp")
    me_z, me_x, me_t = lax.axis_index("kv"), lax.axis_index("dp"), lax.axis_index("tp")
    heads, kv_heads = query_weight.shape[1] // HEAD, key_weight.shape[1] // HEAD
    blocks = row_count // BLOCK
    rep = heads // kv_heads

    parts = nx // heads
    part_rows = HEAD // parts
    q_share = lax.dynamic_slice(query_weight, (lax.rem(me_x, parts) * part_rows, (me_x // parts) * HEAD), (part_rows, HEAD))
    o_rows = output_weight.shape[0] // nx
    o_share = lax.dynamic_slice(output_weight, (me_x * o_rows, 0), (o_rows, HEAD))
    shares = (q_share, o_share)
    chunks = [
        jnp.concatenate(
            [key_weight[:, g * HEAD : (g + 1) * HEAD], value_weight[:, g * HEAD : (g + 1) * HEAD], shares[g]], axis=0
        )
        for g in range(kv_heads)
    ]
    half = HEAD // 2
    inverse = THETA ** (-jnp.arange(half, dtype=f32) / half)
    positions = me_z * row_count + jnp.arange(row_count, dtype=jnp.int32)
    angles = positions.astype(f32)[:, None] * inverse[None, :]
    cosine, sine = jnp.cos(angles), jnp.sin(angles)
    cos = jnp.concatenate([cosine, cosine], axis=1)
    sin = jnp.concatenate([-sine, sine], axis=1)

    ids = jnp.arange(n * blocks, dtype=jnp.int32)
    own = me_z * blocks + jnp.arange(blocks, dtype=jnp.int32)
    seen = jnp.any(block_choice[0][:, :, None] == ids[None, None, :], axis=1) | (own[:, None] == ids[None, :])
    bias = jnp.where(seen, 0.0, NEGATIVE).astype(f32)
    bias = jnp.repeat(bias.reshape(blocks * n, blocks), BLOCK, axis=1)

    z_id = me_z.astype(jnp.int32).reshape(1)
    x_id = jnp.stack([me_x, me_t]).astype(jnp.int32)

    got = rings(chunks, "kv")
    kvs, slices = [], []
    for g in range(kv_heads):
        offs = tuple(o for o, _ in got[g])
        kv, part = call(
            functools.partial(kv_kernel, offs, n),
            [((2, row_count, HEAD), bf16), ((n, part_rows if g == 0 else o_rows, HEAD), bf16)],
            [z_id, x, cos, sin] + [a for _, a in got[g]],
            [pltpu.VMEM((width, 2 * HEAD), bf16)],
            flops=2 * row_count * width * 2 * HEAD,
            moved=4 * 2**20,
        )
        kvs.append(kv)
        slices.append(part)

    around_q = rings([slices[0]], "dp")[0]
    ring_kv = rings(kvs, "kv")
    around_o = rings([slices[1]], "dp")[0]

    (q,) = call(
        functools.partial(q_kernel, tuple(o for o, _ in around_q), nx),
        [((kv_heads, blocks, rep * BLOCK, HEAD), bf16)],
        [x_id, x, cos, sin] + [a for _, a in around_q],
        [pltpu.VMEM((n, HEAD, heads * HEAD), bf16)],
        flops=2 * row_count * width * heads * HEAD,
        moved=4 * 2**20,
    )
    w_theirs, w_ours = call(
        functools.partial(order_kernel, tuple(o for o, _ in around_o), nx),
        [((nx * o_rows, n * HEAD // 2), bf16)] * 2,
        [x_id] + [a for _, a in around_o],
        flops=2**20,
        moved=4 * 2**20,
    )

    cuts = sorted({0, *(2 * (n * k // 16) + 1 for k in (3, 5, 7)), n})
    state = [[] for _ in range(kv_heads)]
    for a, b in zip(cuts[:-1], cuts[1:]):
        for g in range(kv_heads):
            here = ring_kv[g][a:b]
            last = b == len(ring_kv[g])
            full = (blocks, rep * BLOCK, HEAD)
            state[g] = call(
                functools.partial(attend_kernel, g, tuple(o for o, _ in here), n, a == 0, last),
                [((row_count, rep * HEAD), bf16)] if last else [(full, f32)] * 3,
                [z_id, bias, q] + list(state[g]) + [arr for _, arr in here],
                [pltpu.VMEM((rep * BLOCK, len(here) * row_count), f32)],
                flops=4 * rep * row_count * row_count * HEAD * len(here) * 2,
                moved=4 * 2**20,
            )
    mixed = [s[0] for s in state]
    wide = w_ours.shape[1]
    term = functools.partial(call, term_kernel, [((row_count, wide), bf16)], flops=2 * row_count * wide * heads * HEAD, moved=4 * 2**20)
    (sent,) = term([z_id] + mixed + [w_theirs])
    arrived = lax.ppermute(sent, "tp", shift("tp", 1))
    (kept,) = term([z_id] + mixed + [w_ours])
    return (kept.astype(f32) + arrived.astype(f32)).astype(bf16)[None]


def solution(mesh):
    return jax.shard_map(
        on_device,
        mesh=mesh,
        in_specs=(
            P(("grp", "dp"), "kv", None),
            P("kv", "tp"),
            P("kv", "tp"),
            P("kv", "tp"),
            P("tp", "kv"),
            P(("grp", "dp"), "kv", None),
        ),
        out_specs=P(("grp", "dp"), "kv", "tp"),
        check_vma=False,
    )
```

```python
import functools

import jax
import jax.numpy as jnp
from jax import lax
from jax.experimental import pallas as pl
from jax.experimental.pallas import tpu as pltpu
from jax.sharding import PartitionSpec as P

HEAD = 128
BLOCK = 64
THETA = 10000.0
NEGATIVE = -1e30
LOG2E = 1.4426950408889634

bf16, f32 = jnp.bfloat16, jnp.float32
VMEM = pl.BlockSpec(memory_space=pltpu.VMEM)
SMEM = pl.BlockSpec(memory_space=pltpu.SMEM)
ANY = pl.BlockSpec(memory_space=pl.ANY)


def call(kernel, outs, specs, args, scratch=(), flops=0, moved=2**22, limit=24):
    return pl.pallas_call(
        kernel,
        out_shape=[jax.ShapeDtypeStruct(s, d) for s, d in outs],
        in_specs=specs,
        out_specs=[VMEM] * len(outs),
        scratch_shapes=list(scratch),
        compiler_params=pltpu.CompilerParams(vmem_limit_bytes=limit * 2**20),
        cost_estimate=pl.CostEstimate(flops=flops, bytes_accessed=moved, transcendentals=0),
    )(*args)


def shift(axis, by):
    n = lax.axis_size(axis)
    return [(i, (i + by) % n) for i in range(n)]


def ring(start, axis):
    n = lax.axis_size(axis)
    got = [(0, start)]
    right = left = start
    for k in range(1, n // 2 + 1):
        right = lax.ppermute(right, axis, shift(axis, 1))
        got.append((-k, right))
        if k < n - k:
            left = lax.ppermute(left, axis, shift(axis, -1))
            got.append((k, left))
    return got


def turned(u, cos, sin):
    return (u * cos + pltpu.roll(u, HEAD // 2, 1) * sin).astype(bf16)


def projected(x, whole, first, w, sems):
    count = sems.shape[0]
    depth = w.shape[0] // count
    fetch = [
        pltpu.make_async_copy(
            whole.at[k * depth : (k + 1) * depth, first : first + w.shape[1]], w.at[k * depth : (k + 1) * depth], sems.at[k]
        )
        for k in range(count)
    ]
    for f in fetch:
        f.start()
    y = None
    for k, f in enumerate(fetch):
        f.wait()
        at = slice(k * depth, (k + 1) * depth)
        part = jnp.dot(x[:, at], w[at], preferred_element_type=f32)
        y = part if y is None else y + part
    return y


def kv_kernel(first, x, whole, cos, sin, out, w, sems):
    groups = out.shape[1]
    y = projected(x, whole, first, w, sems)
    for g in range(groups):
        k = turned(y[:, g * HEAD : (g + 1) * HEAD], cos[...], sin[...])
        v = y[:, (groups + g) * HEAD : (groups + g + 1) * HEAD].astype(bf16)
        out[:, g, 0] = k.reshape(-1, BLOCK, HEAD)
        out[:, g, 1] = v.reshape(-1, BLOCK, HEAD)


def q_kernel(first, x, whole, cos, sin, out, w, sems):
    groups = out.shape[1]
    y = projected(x, whole, first, w, sems)
    rep = w.shape[1] // HEAD // groups
    for h in range(groups * rep):
        u = turned(y[:, h * HEAD : (h + 1) * HEAD], cos[...], sin[...])
        r = h % rep
        out[:, h // rep, r * BLOCK : (r + 1) * BLOCK, :] = u.reshape(-1, BLOCK, HEAD)


def attend_kernel(ids, bias, q, own, pool, out, near, k_ref, v_ref, s_ref, sems):
    blocks, groups, rows = q.shape[0], q.shape[1], q.shape[2]
    slots = near.shape[1]
    keys = s_ref.shape[1]
    listed = slots * BLOCK
    scale = HEAD ** (-0.5) * LOG2E

    def fetch(i, s):
        return pltpu.make_async_copy(pool.at[ids[i, s]], near.at[i, s], sems.at[i, s])

    def start(i, _):
        for s in range(slots):
            fetch(i, s).start()
        return 0

    lax.fori_loop(0, blocks, start, 0)
    for g in range(groups):
        k_ref[g, listed:] = jnp.zeros((keys - listed, HEAD), bf16)
        v_ref[g, listed:] = jnp.zeros((keys - listed, HEAD), bf16)

    def body(i, _):
        for s in range(slots):
            fetch(i, s).wait()
        for g in range(groups):
            for s in range(slots):
                k_ref[g, s * BLOCK : (s + 1) * BLOCK] = near[i, s, g, 0]
                v_ref[g, s * BLOCK : (s + 1) * BLOCK] = near[i, s, g, 1]
            k_ref[g, listed : listed + BLOCK] = own[i, g, 0]
            v_ref[g, listed : listed + BLOCK] = own[i, g, 1]
        col = lax.broadcasted_iota(jnp.int32, (rows, HEAD), 1)
        row = lax.rem(lax.broadcasted_iota(jnp.int32, (rows, HEAD), 0), BLOCK)
        causal = col <= row
        for g in range(groups):
            base = g * rows
            top = None
            for c in range(keys // HEAD):
                at = slice(c * HEAD, (c + 1) * HEAD)
                s = lax.dot_general(q[i, g], k_ref[g, at], (((1,), (1,)), ((), ())), preferred_element_type=f32) * scale
                if c * HEAD < listed:
                    s = s + bias[i, :, at]
                else:
                    s = jnp.where(causal, s, NEGATIVE)
                s_ref[base : base + rows, at] = s
                top = s if top is None else jnp.maximum(top, s)
            top = jnp.max(top, axis=1, keepdims=True)
            total = acc = None
            for c in range(keys // HEAD):
                at = slice(c * HEAD, (c + 1) * HEAD)
                p = jnp.exp2(s_ref[base : base + rows, at] - top)
                total = p if total is None else total + p
                s_ref[base : base + rows, at] = p
            p = s_ref[base : base + rows].astype(bf16)
            acc = jnp.dot(p, v_ref[g], preferred_element_type=f32)
            mixed = (acc / jnp.sum(total, axis=1, keepdims=True)).astype(bf16)
            rep = rows // BLOCK
            for r in range(rep):
                h = g * rep + r
                out[pl.ds(pl.multiple_of(i * BLOCK, BLOCK), BLOCK), h * HEAD : (h + 1) * HEAD] = mixed[r * BLOCK : (r + 1) * BLOCK]
        return 0

    lax.fori_loop(0, blocks, body, 0)


def order_kernel(offsets, n, me, *refs):
    pieces, (theirs, ours) = refs[: len(offsets)], refs[len(offsets) :]
    for off, piece in zip(offsets, pieces):
        src = lax.rem(me[0] + (off + n), n)
        depth = piece.shape[1]
        half = piece.shape[0] // 2
        rows = pl.ds(pl.multiple_of(src * depth, depth), depth)
        for c in range(half):
            theirs[rows, c * HEAD : (c + 1) * HEAD] = piece[(1 - me[1]) * half + c]
            ours[rows, c * HEAD : (c + 1) * HEAD] = piece[me[1] * half + c]


def term_kernel(mixed, w, out):
    out[...] = jnp.dot(mixed[...], w[...], preferred_element_type=f32).astype(bf16)


def on_device(tokens, query_weight, key_weight, value_weight, output_weight, block_choice):
    x = tokens[0]
    row_count, width = x.shape
    n, nx = lax.axis_size("kv"), lax.axis_size("dp")
    me_z, me_x, me_t = lax.axis_index("kv"), lax.axis_index("dp"), lax.axis_index("tp")
    q_width, k_width = query_weight.shape[1], key_weight.shape[1]
    heads, groups = q_width // HEAD, k_width // HEAD
    blocks = row_count // BLOCK
    rep = heads // groups
    slots = block_choice.shape[2]

    whole = lax.all_gather(jnp.concatenate([query_weight, key_weight, value_weight], axis=1), "kv", axis=0, tiled=True)

    half = HEAD // 2
    inverse = THETA ** (-jnp.arange(half, dtype=f32) / half)
    positions = me_z * row_count + jnp.arange(row_count, dtype=jnp.int32)
    angles = positions.astype(f32)[:, None] * inverse[None, :]
    cosine, sine = jnp.cos(angles), jnp.sin(angles)
    cos = jnp.concatenate([cosine, cosine], axis=1)
    sin = jnp.concatenate([-sine, sine], axis=1)
    choice = block_choice[0]
    ids = jnp.maximum(choice, 0)
    bias = jnp.repeat(jnp.where(choice >= 0, 0.0, NEGATIVE).astype(f32), BLOCK, axis=1)[:, None, :]
    x_id = jnp.stack([me_x, me_t]).astype(jnp.int32)

    o_rows = output_weight.shape[0] // nx
    share = lax.dynamic_slice(output_weight, (me_x * o_rows, 0), (o_rows, HEAD))
    part = lax.all_gather(share, "kv", axis=0, tiled=True).reshape(n, o_rows, HEAD)
    around = ring(part, "dp")
    w_theirs, w_ours = call(
        functools.partial(order_kernel, tuple(o for o, _ in around), nx),
        [((nx * o_rows, n * HEAD // 2), bf16)] * 2,
        [SMEM] + [VMEM] * nx,
        [x_id] + [a for _, a in around],
        flops=2**20,
    )

    (own,) = call(
        functools.partial(kv_kernel, q_width),
        [((blocks, groups, 2, BLOCK, HEAD), bf16)],
        [VMEM, ANY, VMEM, VMEM],
        [x, whole, cos, sin],
        [pltpu.VMEM((width, 2 * k_width), bf16), pltpu.SemaphoreType.DMA((4,))],
        limit=58,
        flops=2 * row_count * width * 2 * k_width,
    )
    pool = lax.all_gather(own, "kv", axis=0, tiled=True)
    (q,) = call(
        functools.partial(q_kernel, 0),
        [((blocks, groups, rep * BLOCK, HEAD), bf16)],
        [VMEM, ANY, VMEM, VMEM],
        [x, whole, cos, sin],
        [pltpu.VMEM((width, q_width), bf16), pltpu.SemaphoreType.DMA((4,))],
        limit=58,
        flops=2 * row_count * width * q_width,
    )
    keys = -(-(slots + 1) * BLOCK // HEAD) * HEAD
    (mixed,) = call(
        attend_kernel,
        [((row_count, q_width), bf16)],
        [SMEM, VMEM, VMEM, VMEM, ANY],
        [ids, bias, q, own, pool],
        [
            pltpu.VMEM((blocks, slots, groups, 2, BLOCK, HEAD), bf16),
            pltpu.VMEM((groups, keys, HEAD), bf16),
            pltpu.VMEM((groups, keys, HEAD), bf16),
            pltpu.VMEM((groups * rep * BLOCK, keys), f32),
            pltpu.SemaphoreType.DMA((blocks, slots)),
        ],
        flops=4 * row_count * keys * q_width,
        moved=2**23,
        limit=58,
    )
    wide = w_ours.shape[1]
    term = functools.partial(call, term_kernel, [((row_count, wide), bf16)], [VMEM] * 2, flops=2 * row_count * wide * q_width)
    (sent,) = term([mixed, w_theirs])
    arrived = lax.ppermute(sent, "tp", shift("tp", 1))
    (kept,) = term([mixed, w_ours])
    return (kept.astype(f32) + arrived.astype(f32)).astype(bf16)[None]


def solution(mesh):
    return jax.shard_map(
        on_device,
        mesh=mesh,
        in_specs=(
            P(("grp", "dp"), "kv", None),
            P("kv", "tp"),
            P("kv", "tp"),
            P("kv", "tp"),
            P("tp", "kv"),
            P(("grp", "dp"), "kv", None),
        ),
        out_specs=P(("grp", "dp"), "kv", "tp"),
        check_vma=False,
    )
```

```python
import functools

import jax
import jax.numpy as jnp
from jax import lax
from jax.experimental import pallas as pl
from jax.experimental.pallas import tpu as pltpu
from jax.sharding import PartitionSpec as P

HEAD = 128
BLOCK = 64
THETA = 10000.0
NEGATIVE = -1e30
LOG2E = 1.4426950408889634

bf16, f16, f32 = jnp.bfloat16, jnp.float16, jnp.float32
IN_BOUND, OUT_BOUND = 2.0**18, 2.0**14
VMEM = pl.BlockSpec(memory_space=pltpu.VMEM)
SMEM = pl.BlockSpec(memory_space=pltpu.SMEM)
ANY = pl.BlockSpec(memory_space=pl.ANY)


def call(kernel, outs, specs, args, scratch=(), flops=0, moved=2**22, limit=24):
    return pl.pallas_call(
        kernel,
        out_shape=[jax.ShapeDtypeStruct(s, d) for s, d in outs],
        in_specs=specs,
        out_specs=[VMEM] * len(outs),
        scratch_shapes=list(scratch),
        compiler_params=pltpu.CompilerParams(vmem_limit_bytes=limit * 2**20),
        cost_estimate=pl.CostEstimate(flops=flops, bytes_accessed=moved, transcendentals=0),
    )(*args)


def shift(axis, by):
    n = lax.axis_size(axis)
    return [(i, (i + by) % n) for i in range(n)]


def coded(w, scale):
    return (w.astype(f32) * scale).astype(f16)


def decoded(w, scale):
    return (w.astype(f32) * (1 / scale)).astype(bf16)


def ring(start, axis):
    n = lax.axis_size(axis)
    got = [(0, start)]
    right = left = start
    for k in range(1, n // 2 + 1):
        right = lax.ppermute(right, axis, shift(axis, 1))
        got.append((-k, right))
        if k < n - k:
            left = lax.ppermute(left, axis, shift(axis, -1))
            got.append((k, left))
    return got


def turned(u, cos, sin):
    return (u * cos + pltpu.roll(u, HEAD // 2, 1) * sin).astype(bf16)


def projected(x, parts, w, sems):
    count, tiles = sems.shape
    each = w.shape[0] // count
    for k in range(count):
        for t in range(tiles):
            at = slice(k * each, (k + 1) * each)
            pltpu.make_async_copy(parts.at[at, t], w.at[at, :, t * HEAD : (t + 1) * HEAD], sems.at[k, t]).start()
    y = None
    for k in range(count):
        at = slice(k * each, (k + 1) * each)
        for t in range(tiles):
            pltpu.make_async_copy(parts.at[at, t], w.at[at, :, t * HEAD : (t + 1) * HEAD], sems.at[k, t]).wait()
        rows = w[at].reshape(each * HEAD, tiles * HEAD)
        part = jnp.dot(x[:, k * each * HEAD : (k + 1) * each * HEAD], rows, preferred_element_type=f32)
        y = part if y is None else y + part
    return y


def kv_kernel(x, parts, cos, sin, out, w, sems):
    groups = out.shape[1]
    y = projected(x, parts, w, sems)
    for g in range(groups):
        k = turned(y[:, g * HEAD : (g + 1) * HEAD], cos[...], sin[...])
        v = y[:, (groups + g) * HEAD : (groups + g + 1) * HEAD].astype(bf16)
        out[:, g, 0] = k.reshape(-1, BLOCK, HEAD)
        out[:, g, 1] = v.reshape(-1, BLOCK, HEAD)


def q_kernel(offsets, n, q_rows, me, x, cos, sin, *refs):
    pieces, (out, w) = refs[: len(offsets)], refs[len(offsets) :]
    groups = out.shape[1]
    heads = w.shape[2] // HEAD
    rep = heads // groups
    parts = HEAD // q_rows
    for off, piece in zip(offsets, pieces):
        src = lax.rem(me[0] + (off + n), n)
        t, low = src // parts, lax.rem(src, parts)
        w[:, pl.ds(pl.multiple_of(low * q_rows, q_rows), q_rows), pl.ds(pl.multiple_of(t * HEAD, HEAD), HEAD)] = piece[:, :q_rows]
    y = jnp.dot(x[...], w[...].reshape(w.shape[0] * HEAD, heads * HEAD), preferred_element_type=f32)
    for h in range(heads):
        u = turned(y[:, h * HEAD : (h + 1) * HEAD], cos[...], sin[...])
        r = h % rep
        out[:, h // rep, r * BLOCK : (r + 1) * BLOCK, :] = u.reshape(-1, BLOCK, HEAD)


def attend_kernel(ids, bias, q, own, pool, out, near, k_ref, v_ref, s_ref, sems):
    blocks, groups, rows = q.shape[0], q.shape[1], q.shape[2]
    slots = near.shape[1]
    keys = s_ref.shape[1]
    listed = slots * BLOCK
    scale = HEAD ** (-0.5) * LOG2E

    def fetch(i, s):
        return pltpu.make_async_copy(pool.at[ids[i, s]], near.at[i, s], sems.at[i, s])

    def start(i, _):
        for s in range(slots):
            fetch(i, s).start()
        return 0

    lax.fori_loop(0, blocks, start, 0)
    for g in range(groups):
        k_ref[g, listed:] = jnp.zeros((keys - listed, HEAD), bf16)
        v_ref[g, listed:] = jnp.zeros((keys - listed, HEAD), bf16)

    def body(i, _):
        for s in range(slots):
            fetch(i, s).wait()
        for g in range(groups):
            for s in range(slots):
                k_ref[g, s * BLOCK : (s + 1) * BLOCK] = near[i, s, g, 0]
                v_ref[g, s * BLOCK : (s + 1) * BLOCK] = near[i, s, g, 1]
            k_ref[g, listed : listed + BLOCK] = own[i, g, 0]
            v_ref[g, listed : listed + BLOCK] = own[i, g, 1]
        col = lax.broadcasted_iota(jnp.int32, (rows, HEAD), 1)
        row = lax.rem(lax.broadcasted_iota(jnp.int32, (rows, HEAD), 0), BLOCK)
        causal = col <= row
        for g in range(groups):
            base = g * rows
            top = None
            for c in range(keys // HEAD):
                at = slice(c * HEAD, (c + 1) * HEAD)
                s = lax.dot_general(q[i, g], k_ref[g, at], (((1,), (1,)), ((), ())), preferred_element_type=f32) * scale
                if c * HEAD < listed:
                    s = s + bias[i, :, at]
                else:
                    s = jnp.where(causal, s, NEGATIVE)
                s_ref[base : base + rows, at] = s
                top = s if top is None else jnp.maximum(top, s)
            top = jnp.max(top, axis=1, keepdims=True)
            total = acc = None
            for c in range(keys // HEAD):
                at = slice(c * HEAD, (c + 1) * HEAD)
                p = jnp.exp2(s_ref[base : base + rows, at] - top)
                total = p if total is None else total + p
                s_ref[base : base + rows, at] = p
            p = s_ref[base : base + rows].astype(bf16)
            acc = jnp.dot(p, v_ref[g], preferred_element_type=f32)
            mixed = (acc / jnp.sum(total, axis=1, keepdims=True)).astype(bf16)
            rep = rows // BLOCK
            for r in range(rep):
                h = g * rep + r
                out[pl.ds(pl.multiple_of(i * BLOCK, BLOCK), BLOCK), h * HEAD : (h + 1) * HEAD] = mixed[r * BLOCK : (r + 1) * BLOCK]
        return 0

    lax.fori_loop(0, blocks, body, 0)


def order_kernel(offsets, n, q_rows, me, *refs):
    pieces, (theirs, ours) = refs[: len(offsets)], refs[len(offsets) :]
    for off, piece in zip(offsets, pieces):
        src = lax.rem(me[0] + (off + n), n)
        depth = piece.shape[1] - q_rows
        half = piece.shape[0] // 2
        rows = pl.ds(pl.multiple_of(src * depth, depth), depth)
        for c in range(half):
            theirs[rows, c * HEAD : (c + 1) * HEAD] = piece[(1 - me[1]) * half + c, q_rows:]
            ours[rows, c * HEAD : (c + 1) * HEAD] = piece[me[1] * half + c, q_rows:]


def term_kernel(mixed, w, out):
    out[...] = jnp.dot(mixed[...], w[...], preferred_element_type=f32).astype(bf16)


def on_device(tokens, query_weight, key_weight, value_weight, output_weight, block_choice):
    x = tokens[0]
    row_count, width = x.shape
    n, nx = lax.axis_size("kv"), lax.axis_size("dp")
    me_z, me_x, me_t = lax.axis_index("kv"), lax.axis_index("dp"), lax.axis_index("tp")
    q_width, k_width = query_weight.shape[1], key_weight.shape[1]
    heads, groups = q_width // HEAD, k_width // HEAD
    blocks = row_count // BLOCK
    rep = heads // groups
    slots = block_choice.shape[2]

    parts = nx // heads
    q_rows = HEAD // parts
    o_rows = output_weight.shape[0] // nx
    q_share = lax.dynamic_slice(query_weight, (lax.rem(me_x, parts) * q_rows, (me_x // parts) * HEAD), (q_rows, HEAD))
    o_share = lax.dynamic_slice(output_weight, (me_x * o_rows, 0), (o_rows, HEAD))
    tiles = [w[:, g * HEAD : (g + 1) * HEAD] for w in (key_weight, value_weight) for g in range(groups)]
    packed = jnp.concatenate([coded(t, IN_BOUND) for t in tiles] + [coded(q_share, IN_BOUND), coded(o_share, OUT_BOUND)], axis=0)
    packed = lax.all_gather(packed, "kv", axis=0, tiled=True).reshape(n, -1, HEAD)
    cut = 2 * groups * HEAD
    kv_parts = decoded(packed[:, :cut], IN_BOUND).reshape(n, 2 * groups, HEAD, HEAD)
    part = jnp.concatenate([decoded(packed[:, cut : cut + q_rows], IN_BOUND), decoded(packed[:, cut + q_rows :], OUT_BOUND)], axis=1)

    half = HEAD // 2
    inverse = THETA ** (-jnp.arange(half, dtype=f32) / half)
    positions = me_z * row_count + jnp.arange(row_count, dtype=jnp.int32)
    angles = positions.astype(f32)[:, None] * inverse[None, :]
    cosine, sine = jnp.cos(angles), jnp.sin(angles)
    cos = jnp.concatenate([cosine, cosine], axis=1)
    sin = jnp.concatenate([-sine, sine], axis=1)
    choice = block_choice[0]
    ids = jnp.maximum(choice, 0)
    bias = jnp.repeat(jnp.where(choice >= 0, 0.0, NEGATIVE).astype(f32), BLOCK, axis=1)[:, None, :]
    x_id = jnp.stack([me_x, me_t]).astype(jnp.int32)

    around = ring(part, "dp")
    offsets = tuple(o for o, _ in around)
    pieces = [a for _, a in around]

    (own,) = call(
        kv_kernel,
        [((blocks, groups, 2, BLOCK, HEAD), bf16)],
        [VMEM, ANY, VMEM, VMEM],
        [x, kv_parts, cos, sin],
        [pltpu.VMEM((n, HEAD, 2 * k_width), bf16), pltpu.SemaphoreType.DMA((4, 2 * groups))],
        flops=2 * row_count * width * 2 * k_width,
        limit=58,
    )
    pool = lax.all_gather(own, "kv", axis=0, tiled=True)
    (q,) = call(
        functools.partial(q_kernel, offsets, nx, q_rows),
        [((blocks, groups, rep * BLOCK, HEAD), bf16)],
        [SMEM] + [VMEM] * (3 + nx),
        [x_id, x, cos, sin] + pieces,
        [pltpu.VMEM((n, HEAD, q_width), bf16)],
        flops=2 * row_count * width * q_width,
    )
    w_theirs, w_ours = call(
        functools.partial(order_kernel, offsets, nx, q_rows),
        [((nx * o_rows, n * HEAD // 2), bf16)] * 2,
        [SMEM] + [VMEM] * nx,
        [x_id] + pieces,
        flops=2**20,
    )
    keys = -(-(slots + 1) * BLOCK // HEAD) * HEAD
    (mixed,) = call(
        attend_kernel,
        [((row_count, q_width), bf16)],
        [SMEM, VMEM, VMEM, VMEM, ANY],
        [ids, bias, q, own, pool],
        [
            pltpu.VMEM((blocks, slots, groups, 2, BLOCK, HEAD), bf16),
            pltpu.VMEM((groups, keys, HEAD), bf16),
            pltpu.VMEM((groups, keys, HEAD), bf16),
            pltpu.VMEM((groups * rep * BLOCK, keys), f32),
            pltpu.SemaphoreType.DMA((blocks, slots)),
        ],
        flops=4 * row_count * keys * q_width,
        moved=2**23,
        limit=58,
    )
    wide = w_ours.shape[1]
    term = functools.partial(call, term_kernel, [((row_count, wide), bf16)], [VMEM] * 2, flops=2 * row_count * wide * q_width)
    (sent,) = term([mixed, w_theirs])
    arrived = lax.ppermute(sent, "tp", shift("tp", 1))
    (kept,) = term([mixed, w_ours])
    return (kept.astype(f32) + arrived.astype(f32)).astype(bf16)[None]


def solution(mesh):
    return jax.shard_map(
        on_device,
        mesh=mesh,
        in_specs=(
            P(("grp", "dp"), "kv", None),
            P("kv", "tp"),
            P("kv", "tp"),
            P("kv", "tp"),
            P("tp", "kv"),
            P(("grp", "dp"), "kv", None),
        ),
        out_specs=P(("grp", "dp"), "kv", "tp"),
        check_vma=False,
    )
```

```python
import functools

import jax
import jax.numpy as jnp
from jax import lax
from jax.experimental import pallas as pl
from jax.experimental.pallas import tpu as pltpu
from jax.sharding import PartitionSpec as P

HEAD = 128
BLOCK = 64
THETA = 10000.0
NEGATIVE = -1e30
LOG2E = 1.4426950408889634

bf16, f16, f32 = jnp.bfloat16, jnp.float16, jnp.float32
CODE = 2.0**14
VMEM = pl.BlockSpec(memory_space=pltpu.VMEM)
SMEM = pl.BlockSpec(memory_space=pltpu.SMEM)
ANY = pl.BlockSpec(memory_space=pl.ANY)


def call(kernel, outs, specs, args, scratch=(), flops=0, moved=2**22, limit=24):
    return pl.pallas_call(
        kernel,
        out_shape=[jax.ShapeDtypeStruct(s, d) for s, d in outs],
        in_specs=specs,
        out_specs=[VMEM] * len(outs),
        scratch_shapes=list(scratch),
        compiler_params=pltpu.CompilerParams(vmem_limit_bytes=limit * 2**20),
        cost_estimate=pl.CostEstimate(flops=flops, bytes_accessed=moved, transcendentals=0),
    )(*args)


def shift(axis, by):
    n = lax.axis_size(axis)
    return [(i, (i + by) % n) for i in range(n)]


def ring(start, axis):
    n = lax.axis_size(axis)
    got = [(0, start)]
    right = left = start
    for k in range(1, n // 2 + 1):
        right = lax.ppermute(right, axis, shift(axis, 1))
        got.append((-k, right))
        if k < n - k:
            left = lax.ppermute(left, axis, shift(axis, -1))
            got.append((k, left))
    return got


def turned(u, cos, sin):
    return (u * cos + pltpu.roll(u, HEAD // 2, 1) * sin).astype(bf16)


def pack_kernel(q_rows, me, query, key, value, output, out, sems):
    copies, at = [], 0

    def put(source, rows):
        copies.append(pltpu.make_async_copy(source, out.at[at : at + rows], sems.at[len(copies)]))
        copies[-1].start()
        return at + rows

    for w in (key, value):
        for g in range(w.shape[1] // HEAD):
            at = put(w.at[:, g * HEAD : (g + 1) * HEAD], HEAD)
    parts = HEAD // q_rows
    t, low = me[0] // parts, lax.rem(me[0], parts)
    at = put(query.at[pl.ds(pl.multiple_of(low * q_rows, q_rows), q_rows), pl.ds(pl.multiple_of(t * HEAD, HEAD), HEAD)], q_rows)
    o_rows = out.shape[0] - at
    put(output.at[pl.ds(pl.multiple_of(me[0] * o_rows, o_rows), o_rows), :], o_rows)
    for c in copies:
        c.wait()


def kv_kernel(x, parts, cos, sin, out):
    groups = out.shape[1]
    n, tiles = parts.shape[0], parts.shape[1]
    w = jnp.concatenate([jnp.concatenate([parts[z, t] for t in range(tiles)], axis=1) for z in range(n)], axis=0)
    y = jnp.dot(x[...], w, preferred_element_type=f32)
    for g in range(groups):
        k = turned(y[:, g * HEAD : (g + 1) * HEAD], cos[...], sin[...])
        v = y[:, (groups + g) * HEAD : (groups + g + 1) * HEAD].astype(bf16)
        out[:, g, 0] = k.reshape(-1, BLOCK, HEAD)
        out[:, g, 1] = v.reshape(-1, BLOCK, HEAD)


def q_kernel(offsets, n, q_rows, me, x, cos, sin, *refs):
    pieces, (out, w) = refs[: len(offsets)], refs[len(offsets) :]
    groups = out.shape[1]
    heads = w.shape[2] // HEAD
    rep = heads // groups
    parts = HEAD // q_rows
    for off, piece in zip(offsets, pieces):
        src = lax.rem(me[0] + (off + n), n)
        t, low = src // parts, lax.rem(src, parts)
        w[:, pl.ds(pl.multiple_of(low * q_rows, q_rows), q_rows), pl.ds(pl.multiple_of(t * HEAD, HEAD), HEAD)] = piece[:, :q_rows]
    y = jnp.dot(x[...], w[...].reshape(w.shape[0] * HEAD, heads * HEAD), preferred_element_type=f32)
    for h in range(heads):
        u = turned(y[:, h * HEAD : (h + 1) * HEAD], cos[...], sin[...])
        r = h % rep
        out[:, h // rep, r * BLOCK : (r + 1) * BLOCK, :] = u.reshape(-1, BLOCK, HEAD)


def attend_kernel(choice, q, own, pool, w_theirs, mixed, sent, near, w, s_ref, p_ref, sems):
    blocks, groups, rows = q.shape[0], q.shape[1], q.shape[2]
    slots = choice.shape[1]
    scale = HEAD ** (-0.5) * LOG2E
    cuts = sems.shape[0] - 1
    each = near.shape[0] // cuts
    copies = [
        pltpu.make_async_copy(pool.at[k * each : (k + 1) * each], near.at[k * each : (k + 1) * each], sems.at[k])
        for k in range(cuts)
    ]
    weight = pltpu.make_async_copy(w_theirs, w, sems.at[cuts])
    for c in copies:
        c.start()
    weight.start()
    key = lax.broadcasted_iota(jnp.int32, (BLOCK, rows), 0)
    col = lax.rem(lax.broadcasted_iota(jnp.int32, (BLOCK, rows), 1), BLOCK)
    causal = key <= col
    for c in copies:
        c.wait()

    def one(i):
        ids = [jnp.maximum(choice[i, s], 0) for s in range(slots)]
        flags = [jnp.where(choice[i, s] >= 0, 0.0, NEGATIVE).astype(f32) for s in range(slots)]
        scores, totals = [], []
        for g in range(groups):
            keys = jnp.concatenate([near[ids[s], g, 0] for s in range(slots)] + [own[i, g, 0]], axis=0)
            scores.append(lax.dot_general(keys, q[i, g], (((1,), (1,)), ((), ())), preferred_element_type=f32))
        for g in range(groups):
            top = None
            for s in range(slots + 1):
                at = slice(s * BLOCK, (s + 1) * BLOCK)
                b = scores[g][at]
                if s == slots:
                    b = jnp.where(causal, b, NEGATIVE)
                s_ref[g, at] = b
                t = jnp.max(b.reshape(BLOCK // 8, 8, rows), axis=0) * scale
                if s < slots:
                    t = t + flags[s]
                top = t if top is None else jnp.maximum(top, t)
            top = jnp.max(top, axis=0, keepdims=True)
            total = None
            for s in range(slots + 1):
                at = slice(s * BLOCK, (s + 1) * BLOCK)
                p = jnp.exp2(s_ref[g, at] * scale - (top - flags[s] if s < slots else top))
                t = jnp.sum(p.reshape(BLOCK // 8, 8, rows), axis=0)
                total = t if total is None else total + t
                p_ref[g, at] = p.astype(bf16)
            totals.append(jnp.sum(total, axis=0, keepdims=True))
        for g in range(groups):
            values = jnp.concatenate([near[ids[s], g, 1] for s in range(slots)] + [own[i, g, 1]], axis=0)
            acc = lax.dot_general(p_ref[g], values, (((0,), (0,)), ((), ())), preferred_element_type=f32)
            part = (acc / jnp.transpose(jnp.broadcast_to(totals[g], (rows, rows)))).astype(bf16)
            rep = rows // BLOCK
            for r in range(rep):
                h = g * rep + r
                mixed[pl.ds(pl.multiple_of(i * BLOCK, BLOCK), BLOCK), h * HEAD : (h + 1) * HEAD] = part[r * BLOCK : (r + 1) * BLOCK]

    def body(i, _):
        one(i)
        return 0

    lax.fori_loop(0, blocks, body, 0, unroll=2)
    weight.wait()
    sent[...] = jnp.dot(mixed[...], w[...], preferred_element_type=f32).astype(bf16)


def order_kernel(offsets, n, q_rows, me, *refs):
    pieces, (theirs, ours) = refs[: len(offsets)], refs[len(offsets) :]
    for off, piece in zip(offsets, pieces):
        src = lax.rem(me[0] + (off + n), n)
        depth = piece.shape[1] - q_rows
        half = piece.shape[0] // 2
        rows = pl.ds(pl.multiple_of(src * depth, depth), depth)
        for c in range(half):
            theirs[rows, c * HEAD : (c + 1) * HEAD] = piece[(1 - me[1]) * half + c, q_rows:]
            ours[rows, c * HEAD : (c + 1) * HEAD] = piece[me[1] * half + c, q_rows:]


def term_kernel(mixed, w, out):
    out[...] = jnp.dot(mixed[...], w[...], preferred_element_type=f32).astype(bf16)


def on_device(tokens, query_weight, key_weight, value_weight, output_weight, block_choice):
    x = tokens[0]
    row_count, width = x.shape
    n, nx = lax.axis_size("kv"), lax.axis_size("dp")
    me_z, me_x, me_t = lax.axis_index("kv"), lax.axis_index("dp"), lax.axis_index("tp")
    q_width, k_width = query_weight.shape[1], key_weight.shape[1]
    heads, groups = q_width // HEAD, k_width // HEAD
    blocks = row_count // BLOCK
    rep = heads // groups
    slots = block_choice.shape[2]

    x_id = jnp.stack([me_x, me_t]).astype(jnp.int32)

    q_rows = HEAD * heads // nx
    o_rows = output_weight.shape[0] // nx
    cut = 2 * groups * HEAD
    (packed,) = call(
        functools.partial(pack_kernel, q_rows),
        [((cut + q_rows + o_rows, HEAD), bf16)],
        [SMEM] + [ANY] * 4,
        [x_id, query_weight, key_weight, value_weight, output_weight],
        [pltpu.SemaphoreType.DMA((2 * groups + 2,))],
        limit=58,
    )
    packed = (packed.astype(f32) * CODE).astype(jnp.float16)
    packed = lax.all_gather(packed, "kv", axis=0, tiled=True).reshape(n, -1, HEAD)
    kv_parts = (packed[:, :cut].astype(f32) * (1 / CODE)).astype(bf16).reshape(n, 2 * groups, HEAD, HEAD)
    part = (packed[:, cut:].astype(f32) * (1 / CODE)).astype(bf16)

    half = HEAD // 2
    lane = jnp.arange(HEAD, dtype=jnp.int32)
    inverse = THETA ** (-lax.rem(lane, half).astype(f32) / half)
    positions = me_z * row_count + jnp.arange(row_count, dtype=jnp.int32)
    angles = positions.astype(f32)[:, None] * inverse[None, :]
    cos = jnp.cos(angles)
    sin = jnp.where(lane < half, -1.0, 1.0)[None, :] * jnp.sin(angles)

    around = ring(part, "dp")
    offsets = tuple(o for o, _ in around)
    pieces = [a for _, a in around]

    (own,) = call(
        kv_kernel,
        [((blocks, groups, 2, BLOCK, HEAD), bf16)],
        [VMEM] * 4,
        [x, kv_parts, cos, sin],
        flops=2 * row_count * width * 2 * k_width,
        limit=16,
    )
    pool = lax.all_gather(own, "kv", axis=0, tiled=True)
    (q,) = call(
        functools.partial(q_kernel, offsets, nx, q_rows),
        [((blocks, groups, rep * BLOCK, HEAD), bf16)],
        [SMEM] + [VMEM] * (3 + nx),
        [x_id, x, cos, sin] + pieces,
        [pltpu.VMEM((n, HEAD, q_width), bf16)],
        flops=2 * row_count * width * q_width,
    )
    w_theirs, w_ours = call(
        functools.partial(order_kernel, offsets, nx, q_rows),
        [((nx * o_rows, n * HEAD // 2), bf16)] * 2,
        [SMEM] + [VMEM] * nx,
        [x_id] + pieces,
        flops=2**20,
    )
    keys = (slots + 1) * BLOCK
    wide = w_ours.shape[1]
    mixed, sent = call(
        attend_kernel,
        [((row_count, q_width), bf16), ((row_count, wide), bf16)],
        [SMEM, VMEM, VMEM, ANY, ANY],
        [block_choice[0], q, own, pool, w_theirs],
        [
            pltpu.VMEM(pool.shape, bf16),
            pltpu.VMEM(w_theirs.shape, bf16),
            pltpu.VMEM((groups, keys, rep * BLOCK), f32),
            pltpu.VMEM((groups, keys, rep * BLOCK), bf16),
            pltpu.SemaphoreType.DMA((9,)),
        ],
        flops=4 * row_count * keys * q_width,
        moved=2**23,
        limit=58,
    )
    arrived = lax.ppermute(sent, "tp", shift("tp", 1))
    (kept,) = call(term_kernel, [((row_count, wide), bf16)], [VMEM] * 2, [mixed, w_ours], flops=2 * row_count * wide * q_width)
    return (kept.astype(f32) + arrived.astype(f32)).astype(bf16)[None]


def solution(mesh):
    return jax.shard_map(
        on_device,
        mesh=mesh,
        in_specs=(
            P(("grp", "dp"), "kv", None),
            P("kv", "tp"),
            P("kv", "tp"),
            P("kv", "tp"),
            P("tp", "kv"),
            P(("grp", "dp"), "kv", None),
        ),
        out_specs=P(("grp", "dp"), "kv", "tp"),
        check_vma=False,
    )
```

```python
import functools

import jax
import jax.numpy as jnp
from jax import lax
from jax.experimental import pallas as pl
from jax.experimental.pallas import tpu as pltpu
from jax.sharding import PartitionSpec as P

HEAD = 128
BLOCK = 64
THETA = 10000.0
NEGATIVE = -1e30
LOG2E = 1.4426950408889634

bf16, f16, f32 = jnp.bfloat16, jnp.float16, jnp.float32
CODE = 2.0**14
VMEM = pl.BlockSpec(memory_space=pltpu.VMEM)
SMEM = pl.BlockSpec(memory_space=pltpu.SMEM)
ANY = pl.BlockSpec(memory_space=pl.ANY)


def call(kernel, outs, specs, args, scratch=(), flops=0, moved=2**22, limit=24):
    return pl.pallas_call(
        kernel,
        out_shape=[jax.ShapeDtypeStruct(s, d) for s, d in outs],
        in_specs=specs,
        out_specs=[VMEM] * len(outs),
        scratch_shapes=list(scratch),
        compiler_params=pltpu.CompilerParams(vmem_limit_bytes=limit * 2**20),
        cost_estimate=pl.CostEstimate(flops=flops, bytes_accessed=moved, transcendentals=0),
    )(*args)


def shift(axis, by):
    n = lax.axis_size(axis)
    return [(i, (i + by) % n) for i in range(n)]


def ring(start, axis):
    n = lax.axis_size(axis)
    got = [(0, start)]
    right = left = start
    for k in range(1, n // 2 + 1):
        right = lax.ppermute(right, axis, shift(axis, 1))
        got.append((-k, right))
        if k < n - k:
            left = lax.ppermute(left, axis, shift(axis, -1))
            got.append((k, left))
    return got


def turned(u, cos, sin):
    return (u * cos + pltpu.roll(u, HEAD // 2, 1) * sin).astype(bf16)


def pack_kernel(q_rows, query, key, value, output, out, sems):
    me = lax.axis_index("dp")
    copies, at = [], 0

    def put(source, rows):
        copies.append(pltpu.make_async_copy(source, out.at[at : at + rows], sems.at[len(copies)]))
        copies[-1].start()
        return at + rows

    for w in (key, value):
        for g in range(w.shape[1] // HEAD):
            at = put(w.at[:, g * HEAD : (g + 1) * HEAD], HEAD)
    parts = HEAD // q_rows
    t, low = me // parts, lax.rem(me, parts)
    at = put(query.at[pl.ds(pl.multiple_of(low * q_rows, q_rows), q_rows), pl.ds(pl.multiple_of(t * HEAD, HEAD), HEAD)], q_rows)
    o_rows = out.shape[0] - at
    put(output.at[pl.ds(pl.multiple_of(me * o_rows, o_rows), o_rows), :], o_rows)
    for c in copies:
        c.wait()


def kv_kernel(x, parts, cos, sin, out):
    groups = out.shape[1]
    n, tiles = parts.shape[0], parts.shape[1]
    w = jnp.concatenate([jnp.concatenate([parts[z, t] for t in range(tiles)], axis=1) for z in range(n)], axis=0)
    y = jnp.dot(x[...], w, preferred_element_type=f32)
    for g in range(groups):
        k = turned(y[:, g * HEAD : (g + 1) * HEAD], cos[...], sin[...])
        v = y[:, (groups + g) * HEAD : (groups + g + 1) * HEAD].astype(bf16)
        out[0, g] = k.reshape(-1, BLOCK, HEAD)
        out[1, g] = v.reshape(-1, BLOCK, HEAD)


def q_kernel(offsets, n, q_rows, me, x, cos, sin, *refs):
    pieces, (out, w) = refs[: len(offsets)], refs[len(offsets) :]
    groups = out.shape[1]
    heads = w.shape[2] // HEAD
    rep = heads // groups
    parts = HEAD // q_rows
    for off, piece in zip(offsets, pieces):
        src = lax.rem(me[0] + (off + n), n)
        t, low = src // parts, lax.rem(src, parts)
        w[:, pl.ds(pl.multiple_of(low * q_rows, q_rows), q_rows), pl.ds(pl.multiple_of(t * HEAD, HEAD), HEAD)] = piece[:, :q_rows]
    y = jnp.dot(x[...], w[...].reshape(w.shape[0] * HEAD, heads * HEAD), preferred_element_type=f32)
    for h in range(heads):
        u = turned(y[:, h * HEAD : (h + 1) * HEAD], cos[...], sin[...])
        r = h % rep
        out[:, h // rep, r * BLOCK : (r + 1) * BLOCK, :] = u.reshape(-1, BLOCK, HEAD)


def pairwise(op, items):
    while len(items) > 1:
        items = [op(x, y) for x, y in zip(items[::2], items[1::2])] + items[len(items) // 2 * 2 :]
    return items[0]


def attend_kernel(choice, q, own, pool, w_theirs, mixed, sent, near, w, s_ref, p_ref, sems):
    blocks, groups, rows = q.shape[0], q.shape[1], q.shape[2]
    slots = choice.shape[1]
    scale = HEAD ** (-0.5) * LOG2E
    copies = {}
    for g in range(groups):
        for kind in range(2):
            copies[g, kind] = pltpu.make_async_copy(pool.at[:, kind, g], near.at[g, kind], sems.at[2 * g + kind])
            copies[g, kind].start()
    weight = pltpu.make_async_copy(w_theirs, w, sems.at[2 * groups])
    weight.start()
    key = lax.broadcasted_iota(jnp.int32, (BLOCK, rows), 0)
    col = lax.rem(lax.broadcasted_iota(jnp.int32, (BLOCK, rows), 1), BLOCK)
    causal = key <= col

    def gathered(g, kind, i):
        if i == 0:
            copies[g, kind].wait()
        ids = [jnp.maximum(choice[i, s], 0) for s in range(slots)]
        listed = [near[g, kind, lax.div(b, blocks), lax.rem(b, blocks)] for b in ids]
        return jnp.concatenate(listed + [own[kind, g, i]], axis=0)

    def front(g, i):
        flags = [jnp.where(choice[i, s] >= 0, 0.0, NEGATIVE).astype(f32) for s in range(slots)]
        return flags, lax.dot_general(gathered(g, 0, i), q[i, g], (((1,), (1,)), ((), ())), preferred_element_type=f32)

    def softened(turn, flags, scores):
        tops = []
        for s in range(slots + 1):
            at = slice(s * BLOCK, (s + 1) * BLOCK)
            b = scores[at]
            if s == slots:
                b = jnp.where(causal, b, NEGATIVE)
            s_ref[turn, at] = b
            t = pairwise(jnp.maximum, [b[r : r + 8] for r in range(0, BLOCK, 8)]) * scale
            tops.append(t + flags[s] if s < slots else t)
        top = jnp.max(pairwise(jnp.maximum, tops), axis=0, keepdims=True)
        totals = []
        for s in range(slots + 1):
            at = slice(s * BLOCK, (s + 1) * BLOCK)
            p = jnp.exp2(s_ref[turn, at] * scale - (top - flags[s] if s < slots else top))
            totals.append(pairwise(jnp.add, [p[r : r + 8] for r in range(0, BLOCK, 8)]))
            p_ref[turn, at] = p.astype(bf16)
        return jnp.sum(pairwise(jnp.add, totals), axis=0, keepdims=True)

    def back(turn, g, i, total):
        acc = lax.dot_general(p_ref[turn], gathered(g, 1, i), (((0,), (0,)), ((), ())), preferred_element_type=f32)
        part = (acc / jnp.transpose(jnp.broadcast_to(total, (rows, rows)))).astype(bf16)
        rep = rows // BLOCK
        for r in range(rep):
            h = g * rep + r
            mixed[i * BLOCK : (i + 1) * BLOCK, h * HEAD : (h + 1) * HEAD] = part[r * BLOCK : (r + 1) * BLOCK]

    units = [(g, i) for g in range(groups) for i in range(blocks)]
    ahead, behind = front(*units[0]), None
    for k, (g, i) in enumerate(units):
        flags, scores = ahead
        if k + 1 < len(units):
            ahead = front(*units[k + 1])
        total = softened(k % 2, flags, scores)
        if behind is not None:
            back(*behind)
        behind = (k % 2, g, i, total)
    back(*behind)
    weight.wait()
    sent[...] = jnp.dot(mixed[...], w[...], preferred_element_type=f32).astype(bf16)


def order_kernel(offsets, n, q_rows, me, *refs):
    pieces, (theirs, ours) = refs[: len(offsets)], refs[len(offsets) :]
    for off, piece in zip(offsets, pieces):
        src = lax.rem(me[0] + (off + n), n)
        depth = piece.shape[1] - q_rows
        half = piece.shape[0] // 2
        rows = pl.ds(pl.multiple_of(src * depth, depth), depth)
        for c in range(half):
            theirs[rows, c * HEAD : (c + 1) * HEAD] = piece[(1 - me[1]) * half + c, q_rows:]
            ours[rows, c * HEAD : (c + 1) * HEAD] = piece[me[1] * half + c, q_rows:]


def term_kernel(mixed, w, out):
    out[...] = jnp.dot(mixed[...], w[...], preferred_element_type=f32).astype(bf16)


def on_device(tokens, query_weight, key_weight, value_weight, output_weight, block_choice):
    x = tokens[0]
    row_count, width = x.shape
    n, nx = lax.axis_size("kv"), lax.axis_size("dp")
    me_z, me_x, me_t = lax.axis_index("kv"), lax.axis_index("dp"), lax.axis_index("tp")
    q_width, k_width = query_weight.shape[1], key_weight.shape[1]
    heads, groups = q_width // HEAD, k_width // HEAD
    blocks = row_count // BLOCK
    rep = heads // groups
    slots = block_choice.shape[2]

    x_id = jnp.stack([me_x, me_t]).astype(jnp.int32)

    q_rows = HEAD * heads // nx
    o_rows = output_weight.shape[0] // nx
    cut = 2 * groups * HEAD
    (packed,) = call(
        functools.partial(pack_kernel, q_rows),
        [((cut + q_rows + o_rows, HEAD), bf16)],
        [ANY] * 4,
        [query_weight, key_weight, value_weight, output_weight],
        [pltpu.SemaphoreType.DMA((2 * groups + 2,))],
        limit=58,
    )
    packed = (packed.astype(f32) * CODE).astype(jnp.float16)
    packed = lax.all_gather(packed, "kv", axis=0, tiled=True).reshape(n, -1, HEAD)
    kv_parts = (packed[:, :cut].astype(f32) * (1 / CODE)).astype(bf16).reshape(n, 2 * groups, HEAD, HEAD)
    part = (packed[:, cut:].astype(f32) * (1 / CODE)).astype(bf16)

    half = HEAD // 2
    lane = jnp.arange(HEAD, dtype=jnp.int32)
    inverse = THETA ** (-lax.rem(lane, half).astype(f32) / half)
    positions = me_z * row_count + jnp.arange(row_count, dtype=jnp.int32)
    angles = positions.astype(f32)[:, None] * inverse[None, :]
    cos = jnp.cos(angles)
    sin = jnp.where(lane < half, -1.0, 1.0)[None, :] * jnp.sin(angles)

    around = ring(part, "dp")
    offsets = tuple(o for o, _ in around)
    pieces = [a for _, a in around]

    (own,) = call(
        kv_kernel,
        [((2, groups, blocks, BLOCK, HEAD), bf16)],
        [VMEM] * 4,
        [x, kv_parts, cos, sin],
        flops=2 * row_count * width * 2 * k_width,
        limit=16,
    )
    pool = lax.all_gather(own, "kv", axis=0, tiled=False)
    (q,) = call(
        functools.partial(q_kernel, offsets, nx, q_rows),
        [((blocks, groups, rep * BLOCK, HEAD), bf16)],
        [SMEM] + [VMEM] * (3 + nx),
        [x_id, x, cos, sin] + pieces,
        [pltpu.VMEM((n, HEAD, q_width), bf16)],
        flops=2 * row_count * width * q_width,
    )
    w_theirs, w_ours = call(
        functools.partial(order_kernel, offsets, nx, q_rows),
        [((nx * o_rows, n * HEAD // 2), bf16)] * 2,
        [SMEM] + [VMEM] * nx,
        [x_id] + pieces,
        flops=2**20,
    )
    keys = (slots + 1) * BLOCK
    wide = w_ours.shape[1]
    mixed, sent = call(
        attend_kernel,
        [((row_count, q_width), bf16), ((row_count, wide), bf16)],
        [SMEM, VMEM, VMEM, ANY, ANY],
        [block_choice[0], q, own, pool, w_theirs],
        [
            pltpu.VMEM((groups, 2, n, blocks, BLOCK, HEAD), bf16),
            pltpu.VMEM(w_theirs.shape, bf16),
            pltpu.VMEM((2, keys, rep * BLOCK), f32),
            pltpu.VMEM((2, keys, rep * BLOCK), bf16),
            pltpu.SemaphoreType.DMA((2 * groups + 1,)),
        ],
        flops=4 * row_count * keys * q_width,
        moved=2**23,
        limit=58,
    )
    arrived = lax.ppermute(sent, "tp", shift("tp", 1))
    (kept,) = call(term_kernel, [((row_count, wide), bf16)], [VMEM] * 2, [mixed, w_ours], flops=2 * row_count * wide * q_width)
    return (kept.astype(f32) + arrived.astype(f32)).astype(bf16)[None]


def solution(mesh):
    return jax.shard_map(
        on_device,
        mesh=mesh,
        in_specs=(
            P(("grp", "dp"), "kv", None),
            P("kv", "tp"),
            P("kv", "tp"),
            P("kv", "tp"),
            P("tp", "kv"),
            P(("grp", "dp"), "kv", None),
        ),
        out_specs=P(("grp", "dp"), "kv", "tp"),
        check_vma=False,
    )
```

```python
import functools

import jax
import jax.numpy as jnp
from jax import lax
from jax.experimental import pallas as pl
from jax.experimental.pallas import tpu as pltpu
from jax.sharding import PartitionSpec as P

HEAD = 128
BLOCK = 64
THETA = 10000.0
NEGATIVE = -1e30
LOG2E = 1.4426950408889634

bf16, f16, f32 = jnp.bfloat16, jnp.float16, jnp.float32
CODE = 2.0**14
VMEM = pl.BlockSpec(memory_space=pltpu.VMEM)
SMEM = pl.BlockSpec(memory_space=pltpu.SMEM)
ANY = pl.BlockSpec(memory_space=pl.ANY)


def call(kernel, outs, specs, args, scratch=(), flops=0, moved=2**22, limit=24):
    return pl.pallas_call(
        kernel,
        out_shape=[jax.ShapeDtypeStruct(s, d) for s, d in outs],
        in_specs=specs,
        out_specs=[VMEM] * len(outs),
        scratch_shapes=list(scratch),
        compiler_params=pltpu.CompilerParams(vmem_limit_bytes=limit * 2**20),
        cost_estimate=pl.CostEstimate(flops=flops, bytes_accessed=moved, transcendentals=0),
    )(*args)


def shift(axis, by):
    n = lax.axis_size(axis)
    return [(i, (i + by) % n) for i in range(n)]


def turned(u, cos, sin):
    return (u * cos + pltpu.roll(u, HEAD // 2, 1) * sin).astype(bf16)


def pack_kernel(q_rows, query, key, value, output, out, sems):
    me = lax.axis_index("dp")
    copies, at = [], 0

    def put(source, rows):
        copies.append(pltpu.make_async_copy(source, out.at[at : at + rows], sems.at[len(copies)]))
        copies[-1].start()
        return at + rows

    for w in (key, value):
        for g in range(w.shape[1] // HEAD):
            at = put(w.at[:, g * HEAD : (g + 1) * HEAD], HEAD)
    parts = HEAD // q_rows
    t, low = me // parts, lax.rem(me, parts)
    at = put(query.at[pl.ds(pl.multiple_of(low * q_rows, q_rows), q_rows), pl.ds(pl.multiple_of(t * HEAD, HEAD), HEAD)], q_rows)
    o_rows = out.shape[0] - at
    put(output.at[pl.ds(pl.multiple_of(me * o_rows, o_rows), o_rows), :], o_rows)
    for c in copies:
        c.wait()


def kv_kernel(x, parts, cos, sin, out):
    groups = out.shape[1]
    n, tiles = parts.shape[0], parts.shape[1]
    w = jnp.concatenate([jnp.concatenate([parts[z, t] for t in range(tiles)], axis=1) for z in range(n)], axis=0)
    y = jnp.dot(x[...], w, preferred_element_type=f32)
    for g in range(groups):
        k = turned(y[:, g * HEAD : (g + 1) * HEAD], cos[...], sin[...])
        v = y[:, (groups + g) * HEAD : (groups + g + 1) * HEAD].astype(bf16)
        out[0, g] = k.reshape(-1, BLOCK, HEAD)
        out[1, g] = v.reshape(-1, BLOCK, HEAD)


def q_kernel(x, shares, cos, sin, out, w):
    groups = out.shape[1]
    heads = w.shape[2] // HEAD
    rep = heads // groups
    parts = shares.shape[0] // heads
    q_rows = HEAD // parts
    for src in range(shares.shape[0]):
        t, low = src // parts, src % parts
        w[:, low * q_rows : (low + 1) * q_rows, t * HEAD : (t + 1) * HEAD] = shares[src, :, :q_rows]
    y = jnp.dot(x[...], w[...].reshape(w.shape[0] * HEAD, heads * HEAD), preferred_element_type=f32)
    for h in range(heads):
        u = turned(y[:, h * HEAD : (h + 1) * HEAD], cos[...], sin[...])
        r = h % rep
        out[:, h // rep, r * BLOCK : (r + 1) * BLOCK, :] = u.reshape(-1, BLOCK, HEAD)


def pairwise(op, items):
    while len(items) > 1:
        items = [op(x, y) for x, y in zip(items[::2], items[1::2])] + items[len(items) // 2 * 2 :]
    return items[0]


def attend_kernel(choice, q, own, pool, w_theirs, mixed, sent, near, w, s_ref, p_ref, sems):
    blocks, groups, rows = q.shape[0], q.shape[1], q.shape[2]
    slots = choice.shape[1]
    scale = HEAD ** (-0.5) * LOG2E
    copies = {}
    for g in range(groups):
        for kind in range(2):
            copies[g, kind] = pltpu.make_async_copy(pool.at[:, kind, g], near.at[g, kind], sems.at[2 * g + kind])
            copies[g, kind].start()
    weight = pltpu.make_async_copy(w_theirs, w, sems.at[2 * groups])
    weight.start()
    key = lax.broadcasted_iota(jnp.int32, (BLOCK, rows), 0)
    col = lax.rem(lax.broadcasted_iota(jnp.int32, (BLOCK, rows), 1), BLOCK)
    causal = key <= col

    def gathered(g, kind, i):
        if i == 0:
            copies[g, kind].wait()
        ids = [jnp.maximum(choice[i, s], 0) for s in range(slots)]
        listed = [near[g, kind, lax.div(b, blocks), lax.rem(b, blocks)] for b in ids]
        return jnp.concatenate(listed + [own[kind, g, i]], axis=0)

    def front(g, i):
        flags = [jnp.where(choice[i, s] >= 0, 0.0, NEGATIVE).astype(f32) for s in range(slots)]
        return flags, lax.dot_general(gathered(g, 0, i), q[i, g], (((1,), (1,)), ((), ())), preferred_element_type=f32)

    def softened(turn, flags, scores):
        tops = []
        for s in range(slots + 1):
            at = slice(s * BLOCK, (s + 1) * BLOCK)
            b = scores[at]
            if s == slots:
                b = jnp.where(causal, b, NEGATIVE)
            s_ref[turn, at] = b
            t = pairwise(jnp.maximum, [b[r : r + 8] for r in range(0, BLOCK, 8)]) * scale
            tops.append(t + flags[s] if s < slots else t)
        top = jnp.max(pairwise(jnp.maximum, tops), axis=0, keepdims=True)
        totals = []
        for s in range(slots + 1):
            at = slice(s * BLOCK, (s + 1) * BLOCK)
            p = jnp.exp2(s_ref[turn, at] * scale - (top - flags[s] if s < slots else top))
            totals.append(pairwise(jnp.add, [p[r : r + 8] for r in range(0, BLOCK, 8)]))
            p_ref[turn, at] = p.astype(bf16)
        return jnp.sum(pairwise(jnp.add, totals), axis=0, keepdims=True)

    def back(turn, g, i, total):
        acc = lax.dot_general(p_ref[turn], gathered(g, 1, i), (((0,), (0,)), ((), ())), preferred_element_type=f32)
        part = (acc / jnp.transpose(jnp.broadcast_to(total, (rows, rows)))).astype(bf16)
        rep = rows // BLOCK
        for r in range(rep):
            h = g * rep + r
            mixed[i * BLOCK : (i + 1) * BLOCK, h * HEAD : (h + 1) * HEAD] = part[r * BLOCK : (r + 1) * BLOCK]

    units = [(g, i) for g in range(groups) for i in range(blocks)]
    ahead, behind = front(*units[0]), None
    for k, (g, i) in enumerate(units):
        flags, scores = ahead
        if k + 1 < len(units):
            ahead = front(*units[k + 1])
        total = softened(k % 2, flags, scores)
        if behind is not None:
            back(*behind)
        behind = (k % 2, g, i, total)
    back(*behind)
    weight.wait()
    sent[...] = jnp.dot(mixed[...], w[...], preferred_element_type=f32).astype(bf16)


def order_kernel(q_rows, shares, theirs, ours):
    me = lax.axis_index("tp")
    depth = shares.shape[2] - q_rows
    half = shares.shape[1] // 2
    for src in range(shares.shape[0]):
        rows = slice(src * depth, (src + 1) * depth)
        for c in range(half):
            theirs[rows, c * HEAD : (c + 1) * HEAD] = shares[src, (1 - me) * half + c, q_rows:]
            ours[rows, c * HEAD : (c + 1) * HEAD] = shares[src, me * half + c, q_rows:]


def term_kernel(mixed, w, out):
    out[...] = jnp.dot(mixed[...], w[...], preferred_element_type=f32).astype(bf16)


def on_device(tokens, query_weight, key_weight, value_weight, output_weight, block_choice):
    x = tokens[0]
    row_count, width = x.shape
    n, nx = lax.axis_size("kv"), lax.axis_size("dp")
    me_z = lax.axis_index("kv")
    q_width, k_width = query_weight.shape[1], key_weight.shape[1]
    heads, groups = q_width // HEAD, k_width // HEAD
    blocks = row_count // BLOCK
    rep = heads // groups
    slots = block_choice.shape[2]

    q_rows = HEAD * heads // nx
    o_rows = output_weight.shape[0] // nx
    cut = 2 * groups * HEAD
    (packed,) = call(
        functools.partial(pack_kernel, q_rows),
        [((cut + q_rows + o_rows, HEAD), bf16)],
        [ANY] * 4,
        [query_weight, key_weight, value_weight, output_weight],
        [pltpu.SemaphoreType.DMA((2 * groups + 2,))],
        limit=58,
    )
    packed = (packed.astype(f32) * CODE).astype(jnp.float16)
    kv_parts = lax.all_gather(packed[:cut], "kv", axis=0, tiled=True)
    kv_parts = (kv_parts.astype(f32) * (1 / CODE)).astype(bf16).reshape(n, 2 * groups, HEAD, HEAD)

    half = HEAD // 2
    lane = jnp.arange(HEAD, dtype=jnp.int32)
    inverse = THETA ** (-lax.rem(lane, half).astype(f32) / half)
    positions = me_z * row_count + jnp.arange(row_count, dtype=jnp.int32)
    angles = positions.astype(f32)[:, None] * inverse[None, :]
    cos = jnp.cos(angles)
    sin = jnp.where(lane < half, -1.0, 1.0)[None, :] * jnp.sin(angles)

    (own,) = call(
        kv_kernel,
        [((2, groups, blocks, BLOCK, HEAD), bf16)],
        [VMEM] * 4,
        [x, kv_parts, cos, sin],
        flops=2 * row_count * width * 2 * k_width,
        limit=16,
    )
    pool = lax.all_gather(own, "kv", axis=0, tiled=False)
    share, own = lax.optimization_barrier((packed[cut:], own))
    shares = lax.all_gather(lax.all_gather(share, "kv", axis=0, tiled=True), "dp", axis=0, tiled=True)
    shares = (shares.astype(f32) * (1 / CODE)).astype(bf16).reshape(nx, n, q_rows + o_rows, HEAD)
    (q,) = call(
        q_kernel,
        [((blocks, groups, rep * BLOCK, HEAD), bf16)],
        [VMEM] * 4,
        [x, shares, cos, sin],
        [pltpu.VMEM((n, HEAD, q_width), bf16)],
        flops=2 * row_count * width * q_width,
    )
    w_theirs, w_ours = call(
        functools.partial(order_kernel, q_rows),
        [((nx * o_rows, n * HEAD // 2), bf16)] * 2,
        [VMEM],
        [shares],
        flops=2**20,
    )
    keys = (slots + 1) * BLOCK
    wide = w_ours.shape[1]
    mixed, sent = call(
        attend_kernel,
        [((row_count, q_width), bf16), ((row_count, wide), bf16)],
        [SMEM, VMEM, VMEM, ANY, ANY],
        [block_choice[0], q, own, pool, w_theirs],
        [
            pltpu.VMEM((groups, 2, n, blocks, BLOCK, HEAD), bf16),
            pltpu.VMEM(w_theirs.shape, bf16),
            pltpu.VMEM((2, keys, rep * BLOCK), f32),
            pltpu.VMEM((2, keys, rep * BLOCK), bf16),
            pltpu.SemaphoreType.DMA((2 * groups + 1,)),
        ],
        flops=4 * row_count * keys * q_width,
        moved=2**23,
        limit=58,
    )
    arrived = lax.ppermute(sent, "tp", shift("tp", 1))
    (kept,) = call(term_kernel, [((row_count, wide), bf16)], [VMEM] * 2, [mixed, w_ours], flops=2 * row_count * wide * q_width)
    return (kept.astype(f32) + arrived.astype(f32)).astype(bf16)[None]


def solution(mesh):
    return jax.shard_map(
        on_device,
        mesh=mesh,
        in_specs=(
            P(("grp", "dp"), "kv", None),
            P("kv", "tp"),
            P("kv", "tp"),
            P("kv", "tp"),
            P("tp", "kv"),
            P(("grp", "dp"), "kv", None),
        ),
        out_specs=P(("grp", "dp"), "kv", "tp"),
        check_vma=False,
    )
```

```python
import functools

import jax
import jax.numpy as jnp
from jax import lax
from jax.experimental import pallas as pl
from jax.experimental.pallas import tpu as pltpu
from jax.sharding import PartitionSpec as P

HEAD = 128
BLOCK = 64
THETA = 10000.0
NEGATIVE = -1e30
LOG2E = 1.4426950408889634

bf16, f16, f32 = jnp.bfloat16, jnp.float16, jnp.float32
CODE_IN, CODE_OUT = 2.0**18, 2.0**14
VMEM = pl.BlockSpec(memory_space=pltpu.VMEM)
SMEM = pl.BlockSpec(memory_space=pltpu.SMEM)
ANY = pl.BlockSpec(memory_space=pl.ANY)


def call(kernel, outs, specs, args, scratch=(), flops=0, moved=2**22, limit=24):
    return pl.pallas_call(
        kernel,
        out_shape=[jax.ShapeDtypeStruct(s, d) for s, d in outs],
        in_specs=specs,
        out_specs=[VMEM] * len(outs),
        scratch_shapes=list(scratch),
        compiler_params=pltpu.CompilerParams(vmem_limit_bytes=limit * 2**20),
        cost_estimate=pl.CostEstimate(flops=flops, bytes_accessed=moved, transcendentals=0),
    )(*args)


def shift(axis, by):
    n = lax.axis_size(axis)
    return [(i, (i + by) % n) for i in range(n)]


def turned(u, cos, sin):
    return (u * cos + pltpu.roll(u, HEAD // 2, 1) * sin).astype(bf16)


def pack_kernel(q_rows, query, key, value, output, out, sems):
    me = lax.axis_index("dp")
    copies, at = [], 0

    def put(source, rows):
        copies.append(pltpu.make_async_copy(source, out.at[at : at + rows], sems.at[len(copies)]))
        copies[-1].start()
        return at + rows

    for w in (key, value):
        for g in range(w.shape[1] // HEAD):
            at = put(w.at[:, g * HEAD : (g + 1) * HEAD], HEAD)
    parts = HEAD // q_rows
    t, low = me // parts, lax.rem(me, parts)
    at = put(query.at[pl.ds(pl.multiple_of(low * q_rows, q_rows), q_rows), pl.ds(pl.multiple_of(t * HEAD, HEAD), HEAD)], q_rows)
    o_rows = out.shape[0] - at
    put(output.at[pl.ds(pl.multiple_of(me * o_rows, o_rows), o_rows), :], o_rows)
    for c in copies:
        c.wait()


def kv_kernel(x, parts, cos, sin, out):
    groups = out.shape[1]
    n, tiles = parts.shape[0], parts.shape[1]
    w = jnp.concatenate([jnp.concatenate([parts[z, t] for t in range(tiles)], axis=1) for z in range(n)], axis=0)
    y = jnp.dot(x[...], w, preferred_element_type=f32)
    for g in range(groups):
        k = turned(y[:, g * HEAD : (g + 1) * HEAD], cos[...], sin[...])
        v = y[:, (groups + g) * HEAD : (groups + g + 1) * HEAD].astype(bf16)
        out[0, g] = k.reshape(-1, BLOCK, HEAD)
        out[1, g] = v.reshape(-1, BLOCK, HEAD)


def q_kernel(x, shares, cos, sin, out, w):
    groups = out.shape[1]
    heads = w.shape[2] // HEAD
    rep = heads // groups
    parts = shares.shape[0] // heads
    q_rows = HEAD // parts
    for src in range(shares.shape[0]):
        t, low = src // parts, src % parts
        w[:, low * q_rows : (low + 1) * q_rows, t * HEAD : (t + 1) * HEAD] = shares[src, :, :q_rows]
    y = jnp.dot(x[...], w[...].reshape(w.shape[0] * HEAD, heads * HEAD), preferred_element_type=f32)
    for h in range(heads):
        u = turned(y[:, h * HEAD : (h + 1) * HEAD], cos[...], sin[...])
        r = h % rep
        out[:, h // rep, r * BLOCK : (r + 1) * BLOCK, :] = u.reshape(-1, BLOCK, HEAD)


def pairwise(op, items):
    while len(items) > 1:
        items = [op(x, y) for x, y in zip(items[::2], items[1::2])] + items[len(items) // 2 * 2 :]
    return items[0]


def attend_kernel(choice, q, own, pool, mixed, near, s_ref, p_ref, sems):
    blocks, groups, rows = q.shape[0], q.shape[1], q.shape[2]
    slots = choice.shape[1]
    scale = HEAD ** (-0.5) * LOG2E
    copies = {}
    for g in range(groups):
        for kind in range(2):
            copies[g, kind] = pltpu.make_async_copy(pool.at[:, kind, g], near.at[g, kind], sems.at[2 * g + kind])
            copies[g, kind].start()
    key = lax.broadcasted_iota(jnp.int32, (BLOCK, rows), 0)
    col = lax.rem(lax.broadcasted_iota(jnp.int32, (BLOCK, rows), 1), BLOCK)
    causal = key <= col

    def gathered(g, kind, i):
        if i == 0:
            copies[g, kind].wait()
        ids = [jnp.maximum(choice[i, s], 0) for s in range(slots)]
        listed = [near[g, kind, lax.div(b, blocks), lax.rem(b, blocks)] for b in ids]
        return jnp.concatenate(listed + [own[kind, g, i]], axis=0)

    def front(g, i):
        flags = [jnp.where(choice[i, s] >= 0, 0.0, NEGATIVE).astype(f32) for s in range(slots)]
        return flags, lax.dot_general(gathered(g, 0, i), q[i, g], (((1,), (1,)), ((), ())), preferred_element_type=f32)

    def softened(turn, flags, scores):
        tops = []
        for s in range(slots + 1):
            at = slice(s * BLOCK, (s + 1) * BLOCK)
            b = scores[at]
            if s == slots:
                b = jnp.where(causal, b, NEGATIVE)
            s_ref[turn, at] = b
            t = pairwise(jnp.maximum, [b[r : r + 8] for r in range(0, BLOCK, 8)]) * scale
            tops.append(t + flags[s] if s < slots else t)
        top = jnp.max(pairwise(jnp.maximum, tops), axis=0, keepdims=True)
        totals = []
        for s in range(slots + 1):
            at = slice(s * BLOCK, (s + 1) * BLOCK)
            p = jnp.exp2(s_ref[turn, at] * scale - (top - flags[s] if s < slots else top))
            totals.append(pairwise(jnp.add, [p[r : r + 8] for r in range(0, BLOCK, 8)]))
            p_ref[turn, at] = p.astype(bf16)
        return jnp.sum(pairwise(jnp.add, totals), axis=0, keepdims=True)

    def back(turn, g, i, total):
        acc = lax.dot_general(p_ref[turn], gathered(g, 1, i), (((0,), (0,)), ((), ())), preferred_element_type=f32)
        part = (acc / jnp.transpose(jnp.broadcast_to(total, (rows, rows)))).astype(bf16)
        rep = rows // BLOCK
        for r in range(rep):
            h = g * rep + r
            mixed[i * BLOCK : (i + 1) * BLOCK, h * HEAD : (h + 1) * HEAD] = part[r * BLOCK : (r + 1) * BLOCK]

    units = [(g, i) for g in range(groups) for i in range(blocks)]
    ahead, behind = front(*units[0]), None
    for k, (g, i) in enumerate(units):
        flags, scores = ahead
        if k + 1 < len(units):
            ahead = front(*units[k + 1])
        total = softened(k % 2, flags, scores)
        if behind is not None:
            back(*behind)
        behind = (k % 2, g, i, total)
    back(*behind)


def order_kernel(q_rows, shares, theirs, ours):
    me = lax.axis_index("tp")
    depth = shares.shape[2] - q_rows
    half = shares.shape[1] // 2
    for src in range(shares.shape[0]):
        rows = slice(src * depth, (src + 1) * depth)
        for c in range(half):
            theirs[rows, c * HEAD : (c + 1) * HEAD] = shares[src, (1 - me) * half + c, q_rows:]
            ours[rows, c * HEAD : (c + 1) * HEAD] = shares[src, me * half + c, q_rows:]


def term_kernel(mixed, w, out):
    out[...] = jnp.dot(mixed[...], w[...], preferred_element_type=f32).astype(bf16)


def last_kernel(mixed, w, kept, out):
    term = jnp.dot(mixed[...], w[...], preferred_element_type=f32).astype(bf16)
    out[...] = (kept[...].astype(f32) + term.astype(f32)).astype(bf16)


def on_device(tokens, query_weight, key_weight, value_weight, output_weight, block_choice):
    x = tokens[0]
    row_count, width = x.shape
    n, nx = lax.axis_size("kv"), lax.axis_size("dp")
    me_z = lax.axis_index("kv")
    q_width, k_width = query_weight.shape[1], key_weight.shape[1]
    heads, groups = q_width // HEAD, k_width // HEAD
    blocks = row_count // BLOCK
    rep = heads // groups
    slots = block_choice.shape[2]

    q_rows = HEAD * heads // nx
    o_rows = output_weight.shape[0] // nx
    cut = 2 * groups * HEAD
    (packed,) = call(
        functools.partial(pack_kernel, q_rows),
        [((cut + q_rows + o_rows, HEAD), bf16)],
        [ANY] * 4,
        [query_weight, key_weight, value_weight, output_weight],
        [pltpu.SemaphoreType.DMA((2 * groups + 2,))],
        limit=58,
    )
    is_out = lax.broadcasted_iota(jnp.int32, packed.shape, 0) >= cut + q_rows
    packed = (packed.astype(f32) * jnp.where(is_out, CODE_OUT, CODE_IN)).astype(jnp.float16)
    kv_parts = lax.all_gather(packed[:cut], "kv", axis=0, tiled=True)
    kv_parts = (kv_parts.astype(f32) * (1 / CODE_IN)).astype(bf16).reshape(n, 2 * groups, HEAD, HEAD)

    half = HEAD // 2
    lane = jnp.arange(HEAD, dtype=jnp.int32)
    inverse = THETA ** (-lax.rem(lane, half).astype(f32) / half)
    positions = me_z * row_count + jnp.arange(row_count, dtype=jnp.int32)
    angles = positions.astype(f32)[:, None] * inverse[None, :]
    cos = jnp.cos(angles)
    sin = jnp.where(lane < half, -1.0, 1.0)[None, :] * jnp.sin(angles)

    (own,) = call(
        kv_kernel,
        [((2, groups, blocks, BLOCK, HEAD), bf16)],
        [VMEM] * 4,
        [x, kv_parts, cos, sin],
        flops=2 * row_count * width * 2 * k_width,
        limit=16,
    )
    pool = lax.all_gather(own, "kv", axis=0, tiled=False)
    share, own = lax.optimization_barrier((packed[cut:], own))
    shares = lax.all_gather(lax.all_gather(share, "kv", axis=0, tiled=True), "dp", axis=0, tiled=True)
    is_out = lax.rem(lax.broadcasted_iota(jnp.int32, shares.shape, 0), q_rows + o_rows) >= q_rows
    shares = (shares.astype(f32) * jnp.where(is_out, 1 / CODE_OUT, 1 / CODE_IN)).astype(bf16)
    shares = shares.reshape(nx, n, q_rows + o_rows, HEAD)
    (q,) = call(
        q_kernel,
        [((blocks, groups, rep * BLOCK, HEAD), bf16)],
        [VMEM] * 4,
        [x, shares, cos, sin],
        [pltpu.VMEM((n, HEAD, q_width), bf16)],
        flops=2 * row_count * width * q_width,
    )
    w_theirs, w_ours = call(
        functools.partial(order_kernel, q_rows),
        [((nx * o_rows, n * HEAD // 2), bf16)] * 2,
        [VMEM],
        [shares],
        flops=2**20,
    )
    w_cross = lax.ppermute(w_theirs, "tp", shift("tp", 1))
    keys = (slots + 1) * BLOCK
    wide = w_ours.shape[1]
    (mixed,) = call(
        attend_kernel,
        [((row_count, q_width), bf16)],
        [SMEM, VMEM, VMEM, ANY],
        [block_choice[0], q, own, pool],
        [
            pltpu.VMEM((groups, 2, n, blocks, BLOCK, HEAD), bf16),
            pltpu.VMEM((2, keys, rep * BLOCK), f32),
            pltpu.VMEM((2, keys, rep * BLOCK), bf16),
            pltpu.SemaphoreType.DMA((2 * groups,)),
        ],
        flops=4 * row_count * keys * q_width,
        moved=2**23,
        limit=58,
    )
    other = lax.ppermute(mixed, "tp", shift("tp", 1))
    result, flops = [((row_count, wide), bf16)], 2 * row_count * wide * q_width
    (kept,) = call(term_kernel, result, [VMEM] * 2, [mixed, w_ours], flops=flops)
    (out,) = call(last_kernel, result, [VMEM] * 3, [other, w_cross, kept], flops=flops)
    return out[None]


def solution(mesh):
    return jax.shard_map(
        on_device,
        mesh=mesh,
        in_specs=(
            P(("grp", "dp"), "kv", None),
            P("kv", "tp"),
            P("kv", "tp"),
            P("kv", "tp"),
            P("tp", "kv"),
            P(("grp", "dp"), "kv", None),
        ),
        out_specs=P(("grp", "dp"), "kv", "tp"),
        check_vma=False,
    )
```

```python
import functools

import jax
import jax.numpy as jnp
from jax import lax
from jax.experimental import pallas as pl
from jax.experimental.pallas import tpu as pltpu
from jax.sharding import PartitionSpec as P

HEAD = 128
BLOCK = 64
THETA = 10000.0
NEGATIVE = -1e30
LOG2E = 1.4426950408889634

bf16, f16, f32 = jnp.bfloat16, jnp.float16, jnp.float32
CODE_IN, CODE_OUT = 2.0**18, 2.0**14
VMEM = pl.BlockSpec(memory_space=pltpu.VMEM)
SMEM = pl.BlockSpec(memory_space=pltpu.SMEM)
ANY = pl.BlockSpec(memory_space=pl.ANY)


def call(kernel, outs, specs, args, scratch=(), flops=0, moved=2**22, limit=24):
    return pl.pallas_call(
        kernel,
        out_shape=[jax.ShapeDtypeStruct(s, d) for s, d in outs],
        in_specs=specs,
        out_specs=[VMEM] * len(outs),
        scratch_shapes=list(scratch),
        compiler_params=pltpu.CompilerParams(vmem_limit_bytes=limit * 2**20),
        cost_estimate=pl.CostEstimate(flops=flops, bytes_accessed=moved, transcendentals=0),
    )(*args)


def shift(axis, by):
    n = lax.axis_size(axis)
    return [(i, (i + by) % n) for i in range(n)]


def turned(u, cos, sin):
    return (u * cos + pltpu.roll(u, HEAD // 2, 1) * sin).astype(bf16)


def pack_kernel(q_rows, query, key, value, output, out, sems):
    me = lax.axis_index("dp")
    copies, at = [], 0

    def put(source, rows):
        copies.append(pltpu.make_async_copy(source, out.at[at : at + rows], sems.at[len(copies)]))
        copies[-1].start()
        return at + rows

    for w in (key, value):
        for g in range(w.shape[1] // HEAD):
            at = put(w.at[:, g * HEAD : (g + 1) * HEAD], HEAD)
    parts = HEAD // q_rows
    t, low = me // parts, lax.rem(me, parts)
    at = put(query.at[pl.ds(pl.multiple_of(low * q_rows, q_rows), q_rows), pl.ds(pl.multiple_of(t * HEAD, HEAD), HEAD)], q_rows)
    o_rows = out.shape[0] - at
    put(output.at[pl.ds(pl.multiple_of(me * o_rows, o_rows), o_rows), :], o_rows)
    for c in copies:
        c.wait()


def kv_kernel(x, parts, cos, sin, out):
    groups = out.shape[1]
    n, tiles = parts.shape[0], parts.shape[1]
    w = jnp.concatenate([jnp.concatenate([parts[z, t] for t in range(tiles)], axis=1) for z in range(n)], axis=0)
    y = jnp.dot(x[...], w, preferred_element_type=f32)
    for g in range(groups):
        k = turned(y[:, g * HEAD : (g + 1) * HEAD], cos[...], sin[...])
        v = y[:, (groups + g) * HEAD : (groups + g + 1) * HEAD].astype(bf16)
        out[0, g] = k.reshape(-1, BLOCK, HEAD)
        out[1, g] = v.reshape(-1, BLOCK, HEAD)


def q_kernel(x, shares, cos, sin, out, w):
    groups = out.shape[1]
    heads = w.shape[2] // HEAD
    rep = heads // groups
    parts = shares.shape[0] // heads
    q_rows = HEAD // parts
    for src in range(shares.shape[0]):
        t, low = src // parts, src % parts
        w[:, low * q_rows : (low + 1) * q_rows, t * HEAD : (t + 1) * HEAD] = shares[src, :, :q_rows]
    y = jnp.dot(x[...], w[...].reshape(w.shape[0] * HEAD, heads * HEAD), preferred_element_type=f32) * (CODE_OUT / CODE_IN)
    for h in range(heads):
        u = turned(y[:, h * HEAD : (h + 1) * HEAD], cos[...], sin[...])
        r = h % rep
        out[:, h // rep, r * BLOCK : (r + 1) * BLOCK, :] = u.reshape(-1, BLOCK, HEAD)


def pairwise(op, items):
    while len(items) > 1:
        items = [op(x, y) for x, y in zip(items[::2], items[1::2])] + items[len(items) // 2 * 2 :]
    return items[0]


def attend_kernel(choice, q, own, pool, mixed, near, s_ref, p_ref, sems):
    blocks, groups, rows = q.shape[0], q.shape[1], q.shape[2]
    slots = choice.shape[1]
    scale = HEAD ** (-0.5) * LOG2E
    copies = {}
    for g in range(groups):
        for kind in range(2):
            copies[g, kind] = pltpu.make_async_copy(pool.at[:, kind, g], near.at[g, kind], sems.at[2 * g + kind])
            copies[g, kind].start()
    key = lax.broadcasted_iota(jnp.int32, (BLOCK, rows), 0)
    col = lax.rem(lax.broadcasted_iota(jnp.int32, (BLOCK, rows), 1), BLOCK)
    causal = key <= col

    def gathered(g, kind, i):
        if i == 0:
            copies[g, kind].wait()
        ids = [jnp.maximum(choice[i, s], 0) for s in range(slots)]
        listed = [near[g, kind, lax.div(b, blocks), lax.rem(b, blocks)] for b in ids]
        return jnp.concatenate(listed + [own[kind, g, i]], axis=0)

    def front(g, i):
        flags = [jnp.where(choice[i, s] >= 0, 0.0, NEGATIVE).astype(f32) for s in range(slots)]
        return flags, lax.dot_general(gathered(g, 0, i), q[i, g], (((1,), (1,)), ((), ())), preferred_element_type=f32)

    def softened(turn, flags, scores):
        tops = []
        for s in range(slots + 1):
            at = slice(s * BLOCK, (s + 1) * BLOCK)
            b = scores[at]
            if s == slots:
                b = jnp.where(causal, b, NEGATIVE)
            s_ref[turn, at] = b
            t = pairwise(jnp.maximum, [b[r : r + 8] for r in range(0, BLOCK, 8)]) * scale
            tops.append(t + flags[s] if s < slots else t)
        top = jnp.max(pairwise(jnp.maximum, tops), axis=0, keepdims=True)
        totals = []
        for s in range(slots + 1):
            at = slice(s * BLOCK, (s + 1) * BLOCK)
            p = jnp.exp2(s_ref[turn, at] * scale - (top - flags[s] if s < slots else top))
            totals.append(pairwise(jnp.add, [p[r : r + 8] for r in range(0, BLOCK, 8)]))
            p_ref[turn, at] = p.astype(bf16)
        return jnp.sum(pairwise(jnp.add, totals), axis=0, keepdims=True)

    def back(turn, g, i, total):
        acc = lax.dot_general(p_ref[turn], gathered(g, 1, i), (((0,), (0,)), ((), ())), preferred_element_type=f32)
        part = (acc / jnp.transpose(jnp.broadcast_to(total, (rows, rows)))).astype(bf16)
        rep = rows // BLOCK
        for r in range(rep):
            h = g * rep + r
            mixed[i * BLOCK : (i + 1) * BLOCK, h * HEAD : (h + 1) * HEAD] = part[r * BLOCK : (r + 1) * BLOCK]

    units = [(g, i) for g in range(groups) for i in range(blocks)]
    ahead, behind = front(*units[0]), None
    for k, (g, i) in enumerate(units):
        flags, scores = ahead
        if k + 1 < len(units):
            ahead = front(*units[k + 1])
        total = softened(k % 2, flags, scores)
        if behind is not None:
            back(*behind)
        behind = (k % 2, g, i, total)
    back(*behind)


def order_kernel(q_rows, shares, theirs, ours):
    me = lax.axis_index("tp")
    depth = shares.shape[2] - q_rows
    half = shares.shape[1] // 2
    for src in range(shares.shape[0]):
        rows = slice(src * depth, (src + 1) * depth)
        for c in range(half):
            theirs[rows, c * HEAD : (c + 1) * HEAD] = shares[src, (1 - me) * half + c, q_rows:]
            ours[rows, c * HEAD : (c + 1) * HEAD] = shares[src, me * half + c, q_rows:]


def term_kernel(mixed, w, out):
    out[...] = jnp.dot(mixed[...], w[...], preferred_element_type=f32).astype(bf16)


def last_kernel(mixed, w, kept, out):
    term = jnp.dot(mixed[...], w[...], preferred_element_type=f32).astype(bf16)
    out[...] = (kept[...].astype(f32) + term.astype(f32)).astype(bf16)


def on_device(tokens, query_weight, key_weight, value_weight, output_weight, block_choice):
    x = tokens[0]
    row_count, width = x.shape
    n, nx = lax.axis_size("kv"), lax.axis_size("dp")
    me_z = lax.axis_index("kv")
    q_width, k_width = query_weight.shape[1], key_weight.shape[1]
    heads, groups = q_width // HEAD, k_width // HEAD
    blocks = row_count // BLOCK
    rep = heads // groups
    slots = block_choice.shape[2]

    q_rows = HEAD * heads // nx
    o_rows = output_weight.shape[0] // nx
    cut = 2 * groups * HEAD
    (packed,) = call(
        functools.partial(pack_kernel, q_rows),
        [((cut + q_rows + o_rows, HEAD), bf16)],
        [ANY] * 4,
        [query_weight, key_weight, value_weight, output_weight],
        [pltpu.SemaphoreType.DMA((2 * groups + 2,))],
        limit=58,
    )
    is_out = lax.broadcasted_iota(jnp.int32, packed.shape, 0) >= cut + q_rows
    packed = (packed.astype(f32) * jnp.where(is_out, CODE_OUT, CODE_IN)).astype(jnp.float16)
    kv_parts = lax.all_gather(packed[:cut], "kv", axis=0, tiled=True)
    kv_parts = (kv_parts.astype(f32) * (1 / CODE_IN)).astype(bf16).reshape(n, 2 * groups, HEAD, HEAD)

    half = HEAD // 2
    lane = jnp.arange(HEAD, dtype=jnp.int32)
    inverse = THETA ** (-lax.rem(lane, half).astype(f32) / half)
    positions = me_z * row_count + jnp.arange(row_count, dtype=jnp.int32)
    angles = positions.astype(f32)[:, None] * inverse[None, :]
    cos = jnp.cos(angles)
    sin = jnp.where(lane < half, -1.0, 1.0)[None, :] * jnp.sin(angles)

    (own,) = call(
        kv_kernel,
        [((2, groups, blocks, BLOCK, HEAD), bf16)],
        [VMEM] * 4,
        [x, kv_parts, cos, sin],
        flops=2 * row_count * width * 2 * k_width,
        limit=16,
    )
    pool = lax.all_gather(own, "kv", axis=0, tiled=False)
    share, own = lax.optimization_barrier((packed[cut:], own))
    shares = lax.all_gather(lax.all_gather(share, "kv", axis=0, tiled=True), "dp", axis=0, tiled=True)
    shares = (shares.astype(f32) * (1 / CODE_OUT)).astype(bf16)
    shares = shares.reshape(nx, n, q_rows + o_rows, HEAD)
    (q,) = call(
        q_kernel,
        [((blocks, groups, rep * BLOCK, HEAD), bf16)],
        [VMEM] * 4,
        [x, shares, cos, sin],
        [pltpu.VMEM((n, HEAD, q_width), bf16)],
        flops=2 * row_count * width * q_width,
    )
    w_theirs, w_ours = call(
        functools.partial(order_kernel, q_rows),
        [((nx * o_rows, n * HEAD // 2), bf16)] * 2,
        [VMEM],
        [shares],
        flops=2**20,
    )
    w_cross = lax.ppermute(w_theirs, "tp", shift("tp", 1))
    keys = (slots + 1) * BLOCK
    wide = w_ours.shape[1]
    (mixed,) = call(
        attend_kernel,
        [((row_count, q_width), bf16)],
        [SMEM, VMEM, VMEM, ANY],
        [block_choice[0], q, own, pool],
        [
            pltpu.VMEM((groups, 2, n, blocks, BLOCK, HEAD), bf16),
            pltpu.VMEM((2, keys, rep * BLOCK), f32),
            pltpu.VMEM((2, keys, rep * BLOCK), bf16),
            pltpu.SemaphoreType.DMA((2 * groups,)),
        ],
        flops=4 * row_count * keys * q_width,
        moved=2**23,
        limit=58,
    )
    other = lax.ppermute(mixed, "tp", shift("tp", 1))
    result, flops = [((row_count, wide), bf16)], 2 * row_count * wide * q_width
    (kept,) = call(term_kernel, result, [VMEM] * 2, [mixed, w_ours], flops=flops)
    (out,) = call(last_kernel, result, [VMEM] * 3, [other, w_cross, kept], flops=flops)
    return out[None]


def solution(mesh):
    return jax.shard_map(
        on_device,
        mesh=mesh,
        in_specs=(
            P(("grp", "dp"), "kv", None),
            P("kv", "tp"),
            P("kv", "tp"),
            P("kv", "tp"),
            P("tp", "kv"),
            P(("grp", "dp"), "kv", None),
        ),
        out_specs=P(("grp", "dp"), "kv", "tp"),
        check_vma=False,
    )
```
